768 devices in a mesh: sp: 12 (over z), tp: 8 (over y), dp: 8 (over x, core).
Axes of the slice: x: 4, y: 8, z: 12, core: 2. Of those that a mesh axis runs over, the one named last changes fastest.
Arguments:
- latents: bfloat16 [8, 6144, 3072], P('dp', ('sp', 'tp')), may hold values from -5 to 5
- condition: bfloat16 [8, 3072], P('dp', ('sp', 'tp')), may hold values from -6 to 6
- context: bfloat16 [8, 384, 3072], P('dp', ('sp', 'tp')), may hold values from -6 to 6
- context_cond: bfloat16 [3072], P(('sp', 'tp')), may hold values from -6 to 6
- shift_weight: bfloat16 [3072, 3072], P(('sp', 'tp')), may hold values from -0.109375 to 0.109375
- scale_weight: bfloat16 [3072, 3072], P(('sp', 'tp')), may hold values from -0.109375 to 0.109375
- out_gate_weight: bfloat16 [3072, 3072], P(('sp', 'tp')), may hold values from -0.109375 to 0.109375
- pre_gain: float32 [3072], replicated, may hold values from 0.1 to 1.9
- post_gain: float32 [3072], replicated, may hold values from 0.1 to 1.9
- query_weight: bfloat16 [3072, 1024], P(None, 'tp'), may hold values from -0.108253175 to 0.108253175
- key_weight: bfloat16 [3072, 256], replicated, may hold values from -0.108253175 to 0.108253175
- value_weight: bfloat16 [3072, 256], replicated, may hold values from -0.109375 to 0.109375
- head_gate_weight: bfloat16 [3072, 1024], P(None, 'tp'), may hold values from -0.109375 to 0.109375
- lambdas: float32 [8], P('tp'), may hold values from 0.3 to 0.8
- head_gain: float32 [128], replicated, may hold values from 0.1 to 1.9
- out_weight: bfloat16 [1024, 3072], P(None, 'tp'), may hold values from -0.1875 to 0.1875
Outputs:
- mixed_out: bfloat16 [8, 6144, 3072], P('dp', ('sp', 'tp'))
The draws below stay inside these ranges and needn't reach their ends.
All inputs are finite; a program needn't handle non-finite values.
Results may differ from the reference program's by a relative error of at most 0.0128.
The reference program's roundings to bfloat16 on the way (of `silu_cond`, `silu_context`, `latent_in`, `context_in`, `weights`, `branch` and `projected`) count: a program that leaves them out, or rounds other values in their place, can miss the bound.
Values may be sent and summed in bfloat16 or wider, within the bound.
No kernel may reach another device: no remote copies, remote signals or barrier semaphores. Data moves between devices by JAX's collectives and lax.ppermute only.
A program may use at most 64 MiB of HBM per device.

```python
import jax
import jax.numpy as jnp
from jax import lax

D = 3072
HEADS = 8
KVH = 2
HQK = 64
HV = 128
CTX = 384
SAMPLES = 8
LAT = 6144


def draw_latents(key, part):
    values = jnp.clip(jax.random.normal(jax.random.fold_in(key, 21), (SAMPLES, LAT, D), jnp.float32), -5.0, 5.0)
    return values.astype(jnp.bfloat16)


def draw_query_weight(key, part):
    values = jnp.clip(jax.random.normal(jax.random.fold_in(key, 31), (D, HEADS * 2 * HQK), jnp.float32), -5.0, 5.0) * D ** (-0.5)
    return values.astype(jnp.bfloat16)


def draw_key_weight(key, part):
    values = jnp.clip(jax.random.normal(jax.random.fold_in(key, 41), (D, KVH * 2 * HQK), jnp.float32), -5.0, 5.0) * D ** (-0.5)
    return values.astype(jnp.bfloat16)


def shard_levels(rng, shape, shards, least, high):
    factor_of, own = 1.0, jax.random.fold_in(rng, 6)
    for dim, shards_of in shards:
        heights = jnp.exp(jax.random.uniform(jax.random.fold_in(own, dim), (shards_of,), jnp.float32, least / len(shards), high / len(shards)))
        factor_of = factor_of * jnp.repeat(heights, shape[dim] // shards_of).reshape([-1 if axis == dim else 1 for axis in range(len(shape))])
    return factor_of


def noise(own_key, extent, scale, most, cuts=(), held_as=jnp.bfloat16):
    drawn = scale * jax.random.normal(own_key, extent, jnp.float32)
    if cuts:
        drawn = drawn * shard_levels(own_key, extent, cuts, -0.22, 0.18)
    return jnp.clip(drawn, -most, most).astype(held_as)


def setup_inputs(seed: int = 0) -> dict:
    key_of = jax.random.split(jax.random.key(seed), 17)
    return {
        "latents": draw_latents(jax.random.fold_in(key_of[16], 71), 0),
        "condition": noise(key_of[1], (SAMPLES, D), 1.0, 6.0, ((0, 8), (1, 96))),
        "context": noise(key_of[2], (SAMPLES, CTX, D), 1.0, 6.0, ((0, 8), (1, 96))),
        "context_cond": noise(key_of[3], (D,), 1.0, 6.0, ((0, 96),)),
        "shift_weight": noise(key_of[4], (D, D), D ** -0.5, 0.109375, ((0, 96),)),
        "scale_weight": noise(key_of[5], (D, D), D ** -0.5, 0.109375, ((0, 96),)),
        "out_gate_weight": noise(key_of[6], (D, D), D ** -0.5, 0.109375, ((0, 96),)),
        "pre_gain": jnp.clip(1.0 + 0.18 * jax.random.normal(key_of[7], (D,), jnp.float32), 0.1, 1.9),
        "post_gain": jnp.clip(1.0 + 0.18 * jax.random.normal(key_of[8], (D,), jnp.float32), 0.1, 1.9),
        "query_weight": draw_query_weight(jax.random.fold_in(key_of[16], 71), 0),
        "key_weight": draw_key_weight(jax.random.fold_in(key_of[16], 71), 0),
        "value_weight": noise(key_of[11], (D, KVH * HV), D ** -0.5, 0.109375),
        "head_gate_weight": noise(key_of[12], (D, HEADS * HV), D ** -0.5, 0.109375, ((1, 8),)),
        "lambdas": jnp.clip(0.3 + 0.5 * jax.random.uniform(key_of[13], (HEADS,), jnp.float32) ** shard_levels(key_of[13], (HEADS,), ((0, 8),), -0.2, 0.2), 0.3, 0.8),
        "head_gain": jnp.clip(1.0 + 0.18 * jax.random.normal(key_of[14], (HV,), jnp.float32), 0.1, 1.9),
        "out_weight": noise(key_of[15], (HEADS * HV, D), (HEADS * HV) ** -0.5, 0.1875, ((1, 8),)),
    }


NORM_EPSILON = 1e-06

def norm_rows(values, norm_gain):
    return values * lax.rsqrt(lax.optimization_barrier(jnp.mean(values * values, axis=-1, keepdims=True)) + NORM_EPSILON) * norm_gain

def rounded(values):
    return lax.optimization_barrier(values.astype(jnp.bfloat16))

def project(tokens, weight):
    flattened = tokens.reshape(-1, tokens.shape[-1])
    result = jnp.dot(flattened, weight, preferred_element_type=jnp.float32)
    return rounded(result).reshape(tokens.shape[:-1] + (weight.shape[1],))

def reference(latents, condition, context, context_cond, shift_weight, scale_weight, out_gate_weight, pre_gain, post_gain, query_weight, key_weight, value_weight, head_gate_weight, lambdas, head_gain, out_weight):
    silu_cond = rounded(jax.nn.silu(condition.astype(jnp.float32)))
    silu_context = rounded(jax.nn.silu(context_cond.astype(jnp.float32)))[None, :]
    shifts = jnp.dot(silu_cond, shift_weight, preferred_element_type=jnp.float32)
    scales = jnp.dot(silu_cond, scale_weight, preferred_element_type=jnp.float32)
    out_gate = jnp.dot(silu_cond, out_gate_weight, preferred_element_type=jnp.float32)
    context_shift = jnp.dot(silu_context, shift_weight, preferred_element_type=jnp.float32)
    context_scale = jnp.dot(silu_context, scale_weight, preferred_element_type=jnp.float32)
    latent_in = rounded(norm_rows(latents.astype(jnp.float32), pre_gain) * (1.0 + scales[:, None, :]) + shifts[:, None, :])
    context_in = rounded(norm_rows(context.astype(jnp.float32), pre_gain) * (1.0 + context_scale[:, None, :]) + context_shift[:, None, :])
    queries = project(latent_in, query_weight).reshape(SAMPLES, LAT, HEADS, 2, HQK)
    head_gate = project(latent_in, head_gate_weight).reshape(SAMPLES, LAT, HEADS, HV)
    joined = jnp.concatenate([context_in, latent_in], axis=1)
    key_rows = project(joined, key_weight).reshape(SAMPLES, CTX + LAT, KVH, 2, HQK)
    value_rows = project(joined, value_weight).reshape(SAMPLES, CTX + LAT, KVH, HV)
    group_size = HEADS // KVH

    def one_head(item_index):
        sample_index = item_index // HEADS
        head_index = item_index % HEADS
        key_group = head_index // group_size
        one_query = queries[sample_index, :, head_index].astype(jnp.float32)
        one_key = key_rows[sample_index, :, key_group].astype(jnp.float32)
        one_value = value_rows[sample_index, :, key_group].astype(jnp.float32)
        scores = jnp.einsum('qmd,kmd->mqk', one_query, one_key) * HQK ** (-0.5)
        largest = lax.optimization_barrier(jnp.max(scores, axis=-1, keepdims=True))
        exponent = jnp.exp(scores - largest)
        normalizer = lax.optimization_barrier(jnp.sum(exponent, axis=-1))
        weights = rounded(exponent).astype(jnp.float32)
        weighted = jnp.einsum('mqk,kv->mqv', weights, one_value)
        ratios = weighted / normalizer[..., None]
        attended = ratios[0] - lambdas[head_index] * ratios[1]
        gate_input = head_gate[sample_index, :, head_index].astype(jnp.float32)
        return rounded(norm_rows(attended, head_gain) * jax.nn.silu(gate_input))
    branch = lax.map(one_head, jnp.arange(SAMPLES * HEADS, dtype=jnp.int32))
    branch = branch.reshape(SAMPLES, HEADS, LAT, HV).transpose(0, 2, 1, 3).reshape(SAMPLES, LAT, HEADS * HV)
    projected = project(branch, out_weight)
    mixed_out = out_gate[:, None, :] * norm_rows(projected.astype(jnp.float32), post_gain)
    return mixed_out.astype(jnp.bfloat16)
```

```python
import jax
import jax.numpy as jnp
from jax import lax
from jax.experimental import pallas as pl
from jax.experimental.pallas import tpu as pltpu
from jax.sharding import PartitionSpec as P

D = 3072
GROUP = 4
HQK = 64
HV = 128
ROWS = 64
CTX_ROWS = 4
TP = 8
SP = 12
QUARTER = 2 * (ROWS + CTX_ROWS)
KEYS = SP * QUARTER
MESSAGE = GROUP * 2 * HV + 2 * HV
CHUNK = 256
VECTOR_ROWS = D // CHUNK
SCALE = HQK ** (-0.5) * 1.4426950408889634
NORM_EPSILON = 1e-06
F32 = jnp.float32
BF16 = jnp.bfloat16
TP_GROUPS = [[0, 1, 2, 3], [4, 5, 6, 7]]
VMEM_LIMIT = 60 * 1024 * 1024


def silu(values):
    return values / (1.0 + jnp.exp(-values))


def partial_sums_kernel(cond_ref, ctx_ref, shift_ref, scale_ref, gate_ref, out_ref):
    both = jnp.concatenate([cond_ref[...], ctx_ref[...]], axis=0).astype(F32)
    both = silu(both).astype(BF16)
    out_ref[...] = jnp.zeros_like(out_ref)
    shift = jnp.dot(both, shift_ref[...], preferred_element_type=F32)
    scale = jnp.dot(both, scale_ref[...], preferred_element_type=F32)
    gate = jnp.dot(both, gate_ref[...], preferred_element_type=F32)
    vectors = [shift[:1], scale[:1], gate[:1], shift[1:], scale[1:]]
    for number, vector in enumerate(vectors):
        for piece in range(VECTOR_ROWS):
            row = number * VECTOR_ROWS + piece
            out_ref[row : row + 1, :] = vector[:, piece * CHUNK : (piece + 1) * CHUNK]


def vector_of(sums_ref, number):
    first = number * VECTOR_ROWS
    return jnp.concatenate(
        [sums_ref[first + piece : first + piece + 1, :] for piece in range(VECTOR_ROWS)], axis=1
    )


def project_kernel(
    quarter_ref, rows_ref, sums_ref, gain_ref, qg_weight_ref, kv_weight_ref,
    q_ref, gate_ref, kv_ref, latent_ref, context_ref,
):
    step = pl.program_id(0)
    gain = gain_ref[...]
    values = rows_ref[0].astype(F32)
    normed = values * lax.rsqrt(jnp.mean(values * values, axis=-1, keepdims=True) + NORM_EPSILON)
    latent = normed[:ROWS] * (gain * (1.0 + vector_of(sums_ref, 1))) + vector_of(sums_ref, 0)
    context = normed[ROWS:] * (gain * (1.0 + vector_of(sums_ref, 4))) + vector_of(sums_ref, 3)
    latent_ref[pl.ds(pl.multiple_of(step * ROWS, ROWS), ROWS), :] = latent.astype(BF16)
    context_ref[step, :CTX_ROWS, :] = context

    @pl.when(step == TP - 1)
    def _():
        projected = jnp.dot(latent_ref[...], qg_weight_ref[...], preferred_element_type=F32)
        q_ref[...] = projected[:, :HV].astype(BF16)
        gate_ref[...] = projected[:, HV:].astype(BF16)
        quarter = quarter_ref[0]
        first = pl.multiple_of(quarter * 2 * ROWS, 2 * ROWS)
        kv = jnp.dot(
            latent_ref[pl.ds(first, 2 * ROWS), :], kv_weight_ref[...], preferred_element_type=F32
        )
        kv_ref[: 2 * ROWS, :] = kv.astype(BF16)
        own_context = jnp.concatenate(
            [context_ref[2 * quarter, :CTX_ROWS, :], context_ref[2 * quarter + 1, :CTX_ROWS, :]],
            axis=0,
        ).astype(BF16)
        kv = jnp.dot(own_context, kv_weight_ref[...], preferred_element_type=F32)
        kv_ref[2 * ROWS :, :] = kv.astype(BF16)


def three_parts(value):
    high = value.astype(BF16)
    rest = value - high.astype(F32)
    middle = rest.astype(BF16)
    low = (rest - middle.astype(F32)).astype(BF16)
    return high.astype(F32), middle.astype(F32), low.astype(F32)


def attention_kernel(lambda_ref, q_ref, kv_ref, gate_ref, out_ref):
    peers = out_ref.shape[0]
    block = peers * ROWS
    q = q_ref[...].reshape(GROUP * block, 2 * HQK)
    keys = kv_ref[:, : 2 * HQK]
    value_rows = kv_ref[:, 2 * HQK :]
    lane = lax.broadcasted_iota(jnp.int32, q.shape, 1)
    stat_lane = lax.broadcasted_iota(jnp.int32, (block, HV), 1)
    stats = jnp.zeros((block, HV), F32)
    for part, piece in enumerate(three_parts(jnp.full((block, HV), lambda_ref[0], F32))):
        stats = jnp.where(stat_lane == part * 32 + 2 * GROUP, piece, stats)
    for m in range(2):
        one_map = jnp.where(lane // HQK == m, q, jnp.zeros_like(q))
        scores = lax.dot_general(
            one_map, keys, (((1,), (1,)), ((), ())), preferred_element_type=F32
        )
        largest = jnp.max(scores, axis=-1, keepdims=True) * SCALE
        exponent = jnp.exp2(scores * SCALE - largest)
        total = jnp.sum(exponent, axis=-1, keepdims=True)
        weighted = jnp.dot(exponent.astype(BF16), value_rows, preferred_element_type=F32)
        ratio = (weighted / total).astype(BF16)
        level = largest + jnp.log2(total)
        for h in range(GROUP):
            column = (2 * h + m) * HV
            for p in range(peers):
                first = h * block + p * ROWS
                out_ref[p, :, column : column + HV] = ratio[first : first + ROWS]
            wide = jnp.broadcast_to(level[h * block : (h + 1) * block], (block, HV))
            for part, piece in enumerate(three_parts(wide)):
                stats = jnp.where(stat_lane == part * 32 + 2 * h + m, piece, stats)
    for p in range(peers):
        out_ref[p, :, 2 * GROUP * HV : 2 * GROUP * HV + HV] = gate_ref[p * ROWS : (p + 1) * ROWS, :]
        out_ref[p, :, 2 * GROUP * HV + HV :] = stats[p * ROWS : (p + 1) * ROWS].astype(BF16)


def finish_kernel(
    parts_ref, weight_ref, sums_ref, post_gain_ref, head_gain_ref, out_ref, branch_ref, projected_ref
):
    step = pl.program_id(0)

    @pl.when(step == 0)
    def _():
        gate_column = 2 * GROUP * HV
        levels = []
        for t in range(TP):
            stats = parts_ref[t, :, gate_column + HV :].astype(F32)
            levels.append(stats[:, :32] + stats[:, 32:64] + stats[:, 64:96])
        for g in range(TP // GROUP):
            members = range(g * GROUP, (g + 1) * GROUP)
            top = levels[members[0]]
            for t in members[1:]:
                top = jnp.maximum(top, levels[t])
            shares = [jnp.exp2(levels[t] - top) for t in members]
            total = shares[0] + shares[1] + shares[2] + shares[3]
            shares = [share / total for share in shares]
            for j in range(GROUP):
                head = g * GROUP + j
                ratios = []
                for m in range(2):
                    index = 2 * j + m
                    ratio = jnp.zeros((ROWS, HV), F32)
                    for t, share in zip(members, shares):
                        part = parts_ref[t, :, index * HV : (index + 1) * HV].astype(F32)
                        ratio = ratio + share[:, index : index + 1] * part
                    ratios.append(ratio)
                own_lambda = levels[head][:, 2 * GROUP : 2 * GROUP + 1]
                attended = ratios[0] - own_lambda * ratios[1]
                square = jnp.mean(attended * attended, axis=-1, keepdims=True)
                gate = parts_ref[head, :, gate_column : gate_column + HV].astype(F32)
                branch = attended * lax.rsqrt(square + NORM_EPSILON) * head_gain_ref[...] * silu(gate)
                branch_ref[:, head * HV : (head + 1) * HV] = branch.astype(BF16)

    projected = jnp.dot(branch_ref[...], weight_ref[0], preferred_element_type=F32)
    projected_ref[step] = projected.astype(BF16).astype(F32)

    @pl.when(step == TP - 1)
    def _():
        square = jnp.zeros((ROWS, 1), F32)
        for t in range(TP):
            square = square + jnp.sum(projected_ref[t] * projected_ref[t], axis=-1, keepdims=True)
        factor = lax.rsqrt(square / D + NORM_EPSILON)
        out_gate = vector_of(sums_ref, 2)
        gain = post_gain_ref[...]
        width = D // TP
        for t in range(TP):
            columns = slice(t * width, (t + 1) * width)
            value = projected_ref[t] * factor * gain[:, columns] * out_gate[:, columns]
            out_ref[:, columns] = value.astype(BF16)


def summed(partials):
    axes = ("sp", "tp")
    pieces = lax.all_to_all(partials, axes, split_axis=0, concat_axis=0, tiled=True)
    own = jnp.sum(pieces, axis=0, keepdims=True)
    copies = jnp.broadcast_to(own, pieces.shape)
    return lax.all_to_all(copies, axes, split_axis=0, concat_axis=0, tiled=True)


def whole_block(shape):
    return pl.BlockSpec(shape, lambda *_: (0,) * len(shape))


def local(
    latents, condition, context, context_cond, shift_weight, scale_weight, out_gate_weight,
    pre_gain, post_gain, query_weight, key_weight, value_weight, head_gate_weight,
    lambdas, head_gain, out_weight,
):
    params = pltpu.CompilerParams(vmem_limit_bytes=VMEM_LIMIT)
    t = lax.axis_index("tp")
    key_group, quarter = t // GROUP, t % GROUP
    with jax.named_scope("gather_rows"):
        rows = jnp.concatenate([latents[0], context[0]], axis=0)
        rows = lax.all_gather(rows, "tp", axis=0, tiled=False)
    with jax.named_scope("modulation"):
        partials = pl.pallas_call(
            partial_sums_kernel,
            out_shape=jax.ShapeDtypeStruct((SP * TP, CHUNK), F32),
            compiler_params=params,
            name="partial_sums",
        )(condition, context_cond[None, :], shift_weight, scale_weight, out_gate_weight)
        sums = summed(partials)
    with jax.named_scope("gather_out_weight"):
        after = out_weight + rows[0, 0, 0] * jnp.zeros((), BF16)
        out_weights = lax.all_gather(after, "tp", axis=0, tiled=False)
    qg_weight = jnp.concatenate([query_weight, head_gate_weight], axis=1)
    kv_weight = jnp.concatenate(
        [
            lax.dynamic_slice_in_dim(key_weight, key_group * 2 * HQK, 2 * HQK, 1),
            lax.dynamic_slice_in_dim(value_weight, key_group * HV, HV, 1),
        ],
        axis=1,
    )
    per_device = ROWS + CTX_ROWS
    with jax.named_scope("project"):
        queries, head_gate, key_values = pl.pallas_call(
            project_kernel,
            grid_spec=pltpu.PrefetchScalarGridSpec(
                num_scalar_prefetch=1,
                grid=(TP,),
                in_specs=[
                    pl.BlockSpec((1, per_device, D), lambda i, _: (i, 0, 0)),
                    whole_block((SP * TP, CHUNK)),
                    whole_block((1, D)),
                    whole_block((D, 2 * HV)),
                    whole_block((D, 2 * HV)),
                ],
                out_specs=[
                    whole_block((TP * ROWS, HV)),
                    whole_block((TP * ROWS, HV)),
                    whole_block((QUARTER, 2 * HV)),
                ],
                scratch_shapes=[
                    pltpu.VMEM((TP * ROWS, D), BF16),
                    pltpu.VMEM((TP, 2 * CTX_ROWS, D), F32),
                ],
            ),
            out_shape=[
                jax.ShapeDtypeStruct((TP * ROWS, HV), BF16),
                jax.ShapeDtypeStruct((TP * ROWS, HV), BF16),
                jax.ShapeDtypeStruct((QUARTER, 2 * HV), BF16),
            ],
            compiler_params=params,
            name="project",
        )(quarter.astype(jnp.int32)[None], rows, sums, pre_gain[None, :], qg_weight, kv_weight)
    with jax.named_scope("gather_keys"):
        key_values = lax.all_gather(key_values, "sp", axis=0, tiled=True)
    with jax.named_scope("exchange_queries"):
        copies = jnp.broadcast_to(queries[None], (GROUP, TP * ROWS, HV))
        copies = lax.all_to_all(
            copies, "tp", split_axis=0, concat_axis=0, axis_index_groups=TP_GROUPS, tiled=True
        )
    peers = 2
    with jax.named_scope("attention"):
        parts = pl.pallas_call(
            attention_kernel,
            grid=(TP // peers,),
            in_specs=[
                pl.BlockSpec(memory_space=pltpu.SMEM),
                pl.BlockSpec((GROUP, peers * ROWS, HV), lambda i: (0, i, 0)),
                whole_block((KEYS, 2 * HV)),
                pl.BlockSpec((peers * ROWS, HV), lambda i: (i, 0)),
            ],
            out_specs=pl.BlockSpec((peers, ROWS, MESSAGE), lambda i: (i, 0, 0)),
            out_shape=jax.ShapeDtypeStruct((TP, ROWS, MESSAGE), BF16),
            compiler_params=params,
            name="attention",
        )(lambdas, copies, key_values, head_gate)
    with jax.named_scope("exchange_parts"):
        parts = lax.all_to_all(parts, "tp", split_axis=0, concat_axis=0, tiled=True)
    with jax.named_scope("finish"):
        mixed_out = pl.pallas_call(
            finish_kernel,
            grid=(TP,),
            in_specs=[
                whole_block((TP, ROWS, MESSAGE)),
                pl.BlockSpec((1, GROUP * 2 * HV, D // TP), lambda i: (i, 0, 0)),
                whole_block((SP * TP, CHUNK)),
                whole_block((1, D)),
                whole_block((1, HV)),
            ],
            out_specs=whole_block((ROWS, D)),
            out_shape=jax.ShapeDtypeStruct((ROWS, D), BF16),
            scratch_shapes=[
                pltpu.VMEM((ROWS, GROUP * 2 * HV), BF16),
                pltpu.VMEM((TP, ROWS, D // TP), F32),
            ],
            compiler_params=params,
            name="finish",
        )(parts, out_weights, sums, post_gain[None, :], head_gain[None, :])
    return mixed_out[None]


def solution(mesh):
    tokens = P("dp", ("sp", "tp"), None)
    channels = P(("sp", "tp"), None)
    return jax.shard_map(
        local,
        mesh=mesh,
        in_specs=(
            tokens, P("dp", ("sp", "tp")), tokens, P(("sp", "tp")), channels, channels, channels,
            P(), P(), P(None, "tp"), P(), P(), P(None, "tp"), P("tp"), P(), P(None, "tp"),
        ),
        out_specs=tokens,
        check_vma=False,
    )
```

```python
import jax
import jax.numpy as jnp
from jax import lax
from jax.experimental import pallas as pl
from jax.experimental.pallas import tpu as pltpu
from jax.sharding import PartitionSpec as P


D = 3072
GROUP = 4
HQK = 64
HV = 128
ROWS = 64
CTX_ROWS = 4
TP = 8
SP = 12
QUARTER = 2 * (ROWS + CTX_ROWS)
KEYS = SP * QUARTER
MESSAGE = GROUP * 2 * HV + 2 * HV
CHUNK = 256
CHAIN = 512
VECTOR_ROWS = D // CHUNK
SCALE = HQK ** (-0.5) * 1.4426950408889634
NORM_EPSILON = 1e-06
F32 = jnp.float32
BF16 = jnp.bfloat16
TP_GROUPS = [[0, 1, 2, 3], [4, 5, 6, 7]]
CORE_PAIRS = [[0, 1], [2, 3], [4, 5], [6, 7]]
VMEM_LIMIT = 60 * 1024 * 1024


def silu(values):
    return values / (1.0 + jnp.exp(-values))


def partial_sums_kernel(cond_ref, ctx_ref, shift_ref, scale_ref, gate_ref, out_ref):
    both = jnp.concatenate([cond_ref[...], ctx_ref[...]], axis=0).astype(F32)
    both = silu(both).astype(BF16)
    out_ref[...] = jnp.zeros_like(out_ref)
    shift = jnp.dot(both, shift_ref[...], preferred_element_type=F32)
    scale = jnp.dot(both, scale_ref[...], preferred_element_type=F32)
    gate = jnp.dot(both, gate_ref[...], preferred_element_type=F32)
    vectors = [shift[:1], scale[:1], gate[:1], shift[1:], scale[1:]]
    for number, vector in enumerate(vectors):
        for piece in range(VECTOR_ROWS):
            row = number * VECTOR_ROWS + piece
            out_ref[row] = vector[:, piece * CHUNK : (piece + 1) * CHUNK]


def vector_of(sums_ref, number):
    first = number * VECTOR_ROWS
    return jnp.concatenate(
        [sums_ref[first + piece] for piece in range(VECTOR_ROWS)], axis=1
    )


def project_kernel(
    quarter_ref, rows_ref, sums_ref, gain_ref, qg_weight_ref, kv_weight_ref,
    q_ref, gate_ref, kv_ref, latent_ref, context_ref,
):
    step = pl.program_id(0)
    pieces = rows_ref.shape[0]
    gain = gain_ref[...]
    latent_scale = gain * (1.0 + vector_of(sums_ref, 1))
    latent_shift = vector_of(sums_ref, 0)
    context_scale = gain * (1.0 + vector_of(sums_ref, 4))
    context_shift = vector_of(sums_ref, 3)
    for piece in range(pieces):
        number = step * pieces + piece
        values = rows_ref[piece].astype(F32)
        square = jnp.mean(values * values, axis=-1, keepdims=True)
        normed = values * lax.rsqrt(square + NORM_EPSILON)
        latent = normed[:ROWS] * latent_scale + latent_shift
        latent_ref[pl.ds(pl.multiple_of(number * ROWS, ROWS), ROWS), :] = latent.astype(BF16)
        context_ref[number, :CTX_ROWS, :] = normed[ROWS:] * context_scale + context_shift

    @pl.when(step == pl.num_programs(0) - 1)
    def _():
        projected = jnp.dot(latent_ref[...], qg_weight_ref[...], preferred_element_type=F32)
        queries = projected[:, :HV].astype(BF16)
        for copy in range(GROUP):
            q_ref[copy] = queries
        gate_ref[...] = projected[:, HV:].astype(BF16)
        quarter = quarter_ref[0]
        first = pl.multiple_of(quarter * 2 * ROWS, 2 * ROWS)
        kv = jnp.dot(
            latent_ref[pl.ds(first, 2 * ROWS), :], kv_weight_ref[...], preferred_element_type=F32
        )
        kv_ref[: 2 * ROWS, :] = kv.astype(BF16)
        own_context = jnp.concatenate(
            [context_ref[2 * quarter, :CTX_ROWS, :], context_ref[2 * quarter + 1, :CTX_ROWS, :]],
            axis=0,
        ).astype(BF16)
        kv = jnp.dot(own_context, kv_weight_ref[...], preferred_element_type=F32)
        kv_ref[2 * ROWS :, :] = kv.astype(BF16)


def three_parts(value):
    high = value.astype(BF16)
    rest = value - high.astype(F32)
    middle = rest.astype(BF16)
    low = (rest - middle.astype(F32)).astype(BF16)
    return high.astype(F32), middle.astype(F32), low.astype(F32)


def attention_kernel(lambda_ref, q_ref, kv_ref, gate_ref, out_ref):
    peers = out_ref.shape[0]
    block = peers * ROWS
    q = q_ref[...].reshape(GROUP * block, 2 * HQK)
    keys = kv_ref[:, : 2 * HQK]
    value_rows = kv_ref[:, 2 * HQK :]
    lane = lax.broadcasted_iota(jnp.int32, (CHAIN, 2 * HQK), 1)
    chains = [(first, m) for first in range(0, GROUP * block, CHAIN) for m in range(2)]

    def scores_of(first, m):
        rows = q[first : first + CHAIN]
        rows = jnp.where(lane // HQK == m, rows, jnp.zeros_like(rows))
        return lax.dot_general(rows, keys, (((1,), (1,)), ((), ())), preferred_element_type=F32)

    def exponent_of(scores):
        largest = jnp.max(scores, axis=-1, keepdims=True) * SCALE
        exponent = jnp.exp2(scores * SCALE - largest)
        return exponent.astype(BF16), jnp.sum(exponent, axis=-1, keepdims=True), largest

    def ratio_of(weights, total, largest):
        weighted = jnp.dot(weights, value_rows, preferred_element_type=F32)
        return (weighted / total).astype(BF16), largest + jnp.log2(total)

    ahead, waiting, ratios, levels = scores_of(*chains[0]), None, {}, {}

    def settle():
        first, m = waiting[0]
        ratio, level = ratio_of(*waiting[1])
        for inner in range(0, CHAIN, block):
            head = (first + inner) // block
            ratios[head, m] = ratio[inner : inner + block]
            levels[head, m] = level[inner : inner + block]

    for number, chain in enumerate(chains):
        scores = ahead
        if number + 1 < len(chains):
            ahead = scores_of(*chains[number + 1])
        exponent = exponent_of(scores)
        if waiting is not None:
            settle()
        waiting = (chain, exponent)
    settle()

    stat_lane = lax.broadcasted_iota(jnp.int32, (block, HV), 1)
    stats = jnp.zeros((block, HV), F32)
    for part, piece in enumerate(three_parts(jnp.full((block, HV), lambda_ref[0], F32))):
        stats = jnp.where(stat_lane == part * 32 + 2 * GROUP, piece, stats)
    for (head, m), ratio in ratios.items():
        column = (2 * head + m) * HV
        for p in range(peers):
            out_ref[p, :, column : column + HV] = ratio[p * ROWS : (p + 1) * ROWS]
        wide = jnp.broadcast_to(levels[head, m], (block, HV))
        for part, piece in enumerate(three_parts(wide)):
            stats = jnp.where(stat_lane == part * 32 + 2 * head + m, piece, stats)
    for p in range(peers):
        out_ref[p, :, 2 * GROUP * HV : 2 * GROUP * HV + HV] = gate_ref[p * ROWS : (p + 1) * ROWS, :]
        out_ref[p, :, 2 * GROUP * HV + HV :] = stats[p * ROWS : (p + 1) * ROWS].astype(BF16)


def finish_kernel(
    parts_ref, weight_ref, sums_ref, post_gain_ref, head_gain_ref, out_ref, branch_ref, projected_ref
):
    step = pl.program_id(0)

    @pl.when(step == 0)
    def _():
        gate_column = 2 * GROUP * HV
        levels = []
        for t in range(TP):
            stats = parts_ref[t, :, gate_column + HV :].astype(F32)
            levels.append(stats[:, :32] + stats[:, 32:64] + stats[:, 64:96])
        for g in range(TP // GROUP):
            members = range(g * GROUP, (g + 1) * GROUP)
            top = levels[members[0]]
            for t in members[1:]:
                top = jnp.maximum(top, levels[t])
            shares = [jnp.exp2(levels[t] - top) for t in members]
            total = shares[0] + shares[1] + shares[2] + shares[3]
            shares = [share / total for share in shares]
            for j in range(GROUP):
                head = g * GROUP + j
                ratios = []
                for m in range(2):
                    index = 2 * j + m
                    ratio = jnp.zeros((ROWS, HV), F32)
                    for t, share in zip(members, shares):
                        part = parts_ref[t, :, index * HV : (index + 1) * HV].astype(F32)
                        ratio = ratio + share[:, index : index + 1] * part
                    ratios.append(ratio)
                own_lambda = levels[head][:, 2 * GROUP : 2 * GROUP + 1]
                attended = ratios[0] - own_lambda * ratios[1]
                square = jnp.mean(attended * attended, axis=-1, keepdims=True)
                gate = parts_ref[head, :, gate_column : gate_column + HV].astype(F32)
                branch = attended * lax.rsqrt(square + NORM_EPSILON) * head_gain_ref[...] * silu(gate)
                branch_ref[:, head * HV : (head + 1) * HV] = branch.astype(BF16)

    half = weight_ref.shape[2]
    pieces = weight_ref.shape[1]
    for piece in range(pieces):
        projected = jnp.dot(branch_ref[:, :half], weight_ref[0, piece], preferred_element_type=F32)
        projected = projected + jnp.dot(
            branch_ref[:, half:], weight_ref[1, piece], preferred_element_type=F32
        )
        projected_ref[step * pieces + piece] = projected.astype(BF16).astype(F32)

    @pl.when(step == pl.num_programs(0) - 1)
    def _():
        square = jnp.zeros((ROWS, 1), F32)
        for t in range(TP):
            square = square + jnp.sum(projected_ref[t] * projected_ref[t], axis=-1, keepdims=True)
        factor = lax.rsqrt(square / D + NORM_EPSILON)
        out_gate = vector_of(sums_ref, 2)
        gain = post_gain_ref[...]
        width = D // TP
        for t in range(TP):
            columns = slice(t * width, (t + 1) * width)
            value = projected_ref[t] * factor * gain[:, columns] * out_gate[:, columns]
            out_ref[:, columns] = value.astype(BF16)


def summed(partials):
    axes = ("sp", "tp")
    pieces = lax.all_to_all(partials, axes, split_axis=0, concat_axis=0, tiled=True)
    own = jnp.sum(pieces, axis=0, keepdims=True)
    copies = jnp.broadcast_to(own, pieces.shape)
    return lax.all_to_all(copies, axes, split_axis=0, concat_axis=0, tiled=True)


def whole_block(shape):
    return pl.BlockSpec(shape, lambda *_: (0,) * len(shape))


def compute(
    latents, condition, context, context_cond, shift_weight, scale_weight, out_gate_weight,
    pre_gain, post_gain, query_weight, key_weight, value_weight, head_gate_weight,
    lambdas, head_gain, out_weight,
):
    params = pltpu.CompilerParams(vmem_limit_bytes=VMEM_LIMIT)
    t = lax.axis_index("tp")
    key_group, quarter = t // GROUP, t % GROUP
    rows = jnp.concatenate([latents[0], context[0]], axis=0)
    rows = lax.all_gather(rows, "tp", axis=0, tiled=False)
    partials = pl.pallas_call(
        partial_sums_kernel,
        out_shape=jax.ShapeDtypeStruct((SP * TP, 1, CHUNK), F32),
        compiler_params=params,
        name="partial_sums",
    )(condition, context_cond[None, :], shift_weight, scale_weight, out_gate_weight)
    sums = summed(partials)
    core = lax.axis_index("dp") % 2
    half = lax.dynamic_slice_in_dim(out_weight, core * GROUP * HV, GROUP * HV, 0)
    half = half + (sums[0, 0, 0] * 0.0).astype(BF16)
    halves = lax.all_gather(half, "tp", axis=0, tiled=False)
    out_weights = lax.all_gather(halves, "dp", axis=0, tiled=False, axis_index_groups=CORE_PAIRS)
    qg_weight = jnp.concatenate([query_weight, head_gate_weight], axis=1)
    kv_weight = jnp.concatenate(
        [
            lax.dynamic_slice_in_dim(key_weight, key_group * 2 * HQK, 2 * HQK, 1),
            lax.dynamic_slice_in_dim(value_weight, key_group * HV, HV, 1),
        ],
        axis=1,
    )
    per_device = ROWS + CTX_ROWS
    queries, head_gate, key_values = pl.pallas_call(
        project_kernel,
        grid_spec=pltpu.PrefetchScalarGridSpec(
            num_scalar_prefetch=1,
            grid=(TP // 2,),
            in_specs=[
                pl.BlockSpec((2, per_device, D), lambda i, _: (i, 0, 0)),
                whole_block((SP * TP, 1, CHUNK)),
                whole_block((1, D)),
                whole_block((D, 2 * HV)),
                whole_block((D, 2 * HV)),
            ],
            out_specs=[
                whole_block((GROUP, TP * ROWS, HV)),
                whole_block((TP * ROWS, HV)),
                whole_block((QUARTER, 2 * HV)),
            ],
            scratch_shapes=[
                pltpu.VMEM((TP * ROWS, D), BF16),
                pltpu.VMEM((TP, 2 * CTX_ROWS, D), F32),
            ],
        ),
        out_shape=[
            jax.ShapeDtypeStruct((GROUP, TP * ROWS, HV), BF16),
            jax.ShapeDtypeStruct((TP * ROWS, HV), BF16),
            jax.ShapeDtypeStruct((QUARTER, 2 * HV), BF16),
        ],
        compiler_params=params,
        name="project",
    )(quarter.astype(jnp.int32)[None], rows, sums, pre_gain[None, :], qg_weight, kv_weight)
    key_values = lax.all_gather(key_values, "sp", axis=0, tiled=True)
    queries = lax.all_to_all(
        queries, "tp", split_axis=0, concat_axis=0, axis_index_groups=TP_GROUPS, tiled=True
    )
    peers = 4
    parts = pl.pallas_call(
        attention_kernel,
        grid=(TP // peers,),
        in_specs=[
            pl.BlockSpec(memory_space=pltpu.SMEM),
            pl.BlockSpec((GROUP, peers * ROWS, HV), lambda i: (0, i, 0)),
            whole_block((KEYS, 2 * HV)),
            pl.BlockSpec((peers * ROWS, HV), lambda i: (i, 0)),
        ],
        out_specs=pl.BlockSpec((peers, ROWS, MESSAGE), lambda i: (i, 0, 0)),
        out_shape=jax.ShapeDtypeStruct((TP, ROWS, MESSAGE), BF16),
        compiler_params=params,
        name="attention",
    )(lambdas, queries, key_values, head_gate)
    parts = lax.all_to_all(parts, "tp", split_axis=0, concat_axis=0, tiled=True)
    mixed_out = pl.pallas_call(
        finish_kernel,
        grid=(TP // 2,),
        in_specs=[
            whole_block((TP, ROWS, MESSAGE)),
            pl.BlockSpec((2, 2, GROUP * HV, D // TP), lambda i: (0, i, 0, 0)),
            whole_block((SP * TP, 1, CHUNK)),
            whole_block((1, D)),
            whole_block((1, HV)),
        ],
        out_specs=whole_block((ROWS, D)),
        out_shape=jax.ShapeDtypeStruct((ROWS, D), BF16),
        scratch_shapes=[
            pltpu.VMEM((ROWS, GROUP * 2 * HV), BF16),
            pltpu.VMEM((TP, ROWS, D // TP), F32),
        ],
        compiler_params=params,
        name="finish",
    )(parts, out_weights, sums, post_gain[None, :], head_gain[None, :])
    return mixed_out[None]


def solution(mesh):
    tokens = P("dp", ("sp", "tp"), None)
    channels = P(("sp", "tp"), None)
    return jax.shard_map(
        compute,
        mesh=mesh,
        in_specs=(
            tokens, P("dp", ("sp", "tp")), tokens, P(("sp", "tp")), channels, channels, channels,
            P(), P(), P(None, "tp"), P(), P(), P(None, "tp"), P("tp"), P(), P(None, "tp"),
        ),
        out_specs=tokens,
        check_vma=False,
    )
```

```python
import jax
import jax.numpy as jnp
from jax import lax
from jax.experimental import pallas as pl
from jax.experimental.pallas import tpu as pltpu
from jax.sharding import PartitionSpec as P


D = 3072
GROUP = 4
HQK = 64
HV = 128
ROWS = 64
CTX_ROWS = 4
TP = 8
SP = 12
QUARTER = 2 * (ROWS + CTX_ROWS)
KEYS = SP * QUARTER
STATS = GROUP * 2
GATE_ROW = STATS * ROWS
STAT_ROW = GATE_ROW + ROWS
MESSAGE = STAT_ROW + 2 * STATS
CHUNK = 256
CHAIN = 512
VECTOR_ROWS = D // CHUNK
SCALE = HQK ** (-0.5) * 1.4426950408889634
NORM_EPSILON = 1e-06
F32 = jnp.float32
BF16 = jnp.bfloat16
TP_GROUPS = [[0, 1, 2, 3], [4, 5, 6, 7]]
VMEM_LIMIT = 60 * 1024 * 1024


def silu(values):
    return values / (1.0 + jnp.exp(-values))


def partial_sums_kernel(cond_ref, ctx_ref, shift_ref, scale_ref, gate_ref, out_ref):
    both = jnp.concatenate([cond_ref[...], ctx_ref[...]], axis=0).astype(F32)
    both = silu(both).astype(BF16)
    out_ref[...] = jnp.zeros_like(out_ref)
    shift = jnp.dot(both, shift_ref[...], preferred_element_type=F32)
    scale = jnp.dot(both, scale_ref[...], preferred_element_type=F32)
    gate = jnp.dot(both, gate_ref[...], preferred_element_type=F32)
    vectors = [shift[:1], scale[:1], gate[:1], shift[1:], scale[1:]]
    for number, vector in enumerate(vectors):
        for piece in range(VECTOR_ROWS):
            row = number * VECTOR_ROWS + piece
            out_ref[row] = vector[:, piece * CHUNK : (piece + 1) * CHUNK]


def vector_of(sums_ref, number):
    first = number * VECTOR_ROWS
    return jnp.concatenate(
        [sums_ref[first + piece] for piece in range(VECTOR_ROWS)], axis=1
    )


def modulated(tokens, scale, shift):
    values = tokens.astype(F32)
    square = jnp.mean(values * values, axis=-1, keepdims=True)
    return (values * lax.rsqrt(square + NORM_EPSILON) * scale + shift).astype(BF16)


def project_kernel(
    place_ref, rows_ref, own_ref, other_ref, sums_ref, gain_ref,
    query_weight_ref, gate_weight_ref, key_weight_ref, value_weight_ref,
    q_ref, gate_ref, kv_ref, latent_ref,
):
    step = pl.program_id(0)
    pieces = rows_ref.shape[0]
    gain = gain_ref[...]
    scale, shift = gain * (1.0 + vector_of(sums_ref, 1)), vector_of(sums_ref, 0)
    for piece in range(pieces):
        first = pl.multiple_of((step * pieces + piece) * ROWS, ROWS)
        latent_ref[pl.ds(first, ROWS), :] = modulated(rows_ref[piece], scale, shift)

    @pl.when(step == pl.num_programs(0) - 1)
    def _():
        weight = jnp.concatenate([query_weight_ref[...], gate_weight_ref[...]], axis=1)
        projected = jnp.dot(latent_ref[...], weight, preferred_element_type=F32)
        queries = projected[:, :HV].astype(BF16)
        for copy in range(GROUP):
            q_ref[copy] = queries
        gate_ref[...] = projected[:, HV:].astype(BF16)
        weight = jnp.concatenate([key_weight_ref[...], value_weight_ref[...]], axis=1)
        first = pl.multiple_of(place_ref[0] * 2 * ROWS, 2 * ROWS)
        kv = jnp.dot(latent_ref[pl.ds(first, 2 * ROWS), :], weight, preferred_element_type=F32)
        kv_ref[: 2 * ROWS, :] = kv.astype(BF16)
        context = jnp.concatenate([own_ref[...].astype(F32), other_ref[...].astype(F32)], axis=0)
        context_scale = gain * (1.0 + vector_of(sums_ref, 4))
        context = modulated(context, context_scale, vector_of(sums_ref, 3))
        kv = jnp.dot(context, weight, preferred_element_type=F32)
        kv_ref[2 * ROWS :, :] = kv.astype(BF16)


def three_parts(value):
    high = value.astype(BF16)
    rest = value - high.astype(F32)
    middle = rest.astype(BF16)
    low = (rest - middle.astype(F32)).astype(BF16)
    return high.astype(F32), middle.astype(F32), low.astype(F32)


def attention_kernel(lambda_ref, q_ref, kv_ref, gate_ref, out_ref):
    peers = out_ref.shape[0]
    block = peers * ROWS
    q = q_ref[...].reshape(GROUP * block, 2 * HQK)
    keys = kv_ref[:, : 2 * HQK]
    value_rows = kv_ref[:, 2 * HQK :]
    lane = lax.broadcasted_iota(jnp.int32, (CHAIN, 2 * HQK), 1)
    chains = [(first, m) for first in range(0, GROUP * block, CHAIN) for m in range(2)]

    def scores_of(first, m):
        rows = q[first : first + CHAIN]
        rows = jnp.where(lane // HQK == m, rows, jnp.zeros_like(rows))
        return lax.dot_general(rows, keys, (((1,), (1,)), ((), ())), preferred_element_type=F32)

    def exponent_of(scores):
        largest = jnp.max(scores, axis=-1, keepdims=True) * SCALE
        exponent = jnp.exp2(scores * SCALE - largest)
        return exponent.astype(BF16), jnp.sum(exponent, axis=-1, keepdims=True), largest

    def ratio_of(weights, total, largest):
        weighted = jnp.dot(weights, value_rows, preferred_element_type=F32)
        return (weighted / total).astype(BF16), largest + jnp.log2(total)

    ahead, waiting, ratios, levels = scores_of(*chains[0]), None, {}, {}

    def settle():
        first, m = waiting[0]
        ratio, level = ratio_of(*waiting[1])
        for inner in range(0, CHAIN, block):
            head = (first + inner) // block
            ratios[head, m] = ratio[inner : inner + block]
            levels[head, m] = level[inner : inner + block]

    for number, chain in enumerate(chains):
        scores = ahead
        if number + 1 < len(chains):
            ahead = scores_of(*chains[number + 1])
        exponent = exponent_of(scores)
        if waiting is not None:
            settle()
        waiting = (chain, exponent)
    settle()

    stat_lane = lax.broadcasted_iota(jnp.int32, (block, HV), 1)
    stats = jnp.zeros((block, HV), F32)
    for (head, m), ratio in ratios.items():
        index = 2 * head + m
        for p in range(peers):
            out_ref[p, index * ROWS : (index + 1) * ROWS, :] = ratio[p * ROWS : (p + 1) * ROWS]
        wide = jnp.broadcast_to(levels[head, m], (block, HV))
        stats = jnp.where(stat_lane == index, wide, stats)
    high, middle, low = three_parts(jnp.transpose(stats)[:STATS])
    row = lax.broadcasted_iota(jnp.int32, (STATS, ROWS), 0)
    own_lambda = jnp.zeros((STATS, ROWS), F32)
    for part, piece in enumerate(three_parts(jnp.full((STATS, ROWS), lambda_ref[0], F32))):
        own_lambda = jnp.where(row == part, piece, own_lambda)
    for p in range(peers):
        lanes = slice(p * ROWS, (p + 1) * ROWS)
        out_ref[p, GATE_ROW:STAT_ROW, :] = gate_ref[lanes, :]
        upper = jnp.concatenate([high[:, lanes], middle[:, lanes]], axis=1)
        lower = jnp.concatenate([low[:, lanes], own_lambda], axis=1)
        out_ref[p, STAT_ROW:, :] = jnp.concatenate([upper, lower], axis=0).astype(BF16)


def finish_kernel(
    core_ref, parts_ref, own_ref, other_ref, sums_ref, post_gain_ref, head_gain_ref,
    out_ref, branch_ref, projected_ref,
):
    step = pl.program_id(0)

    @pl.when(step == 0)
    def _():
        levels, lambdas = [], []
        for t in range(TP):
            stats = parts_ref[t, STAT_ROW:, :].astype(F32)
            upper, lower = stats[:STATS], stats[STATS:]
            levels.append(upper[:, :ROWS] + upper[:, ROWS:] + lower[:, :ROWS])
            lambdas.append(lower[0:1, ROWS:] + lower[1:2, ROWS:] + lower[2:3, ROWS:])
        shares = []
        for g in range(TP // GROUP):
            group = levels[g * GROUP : (g + 1) * GROUP]
            top = jnp.maximum(jnp.maximum(group[0], group[1]), jnp.maximum(group[2], group[3]))
            group = [jnp.exp2(level - top) for level in group]
            total = group[0] + group[1] + group[2] + group[3]
            shares = shares + [share / total for share in group]
        columns = jnp.concatenate(shares + lambdas, axis=0)
        columns = jnp.concatenate([columns, jnp.zeros_like(columns)], axis=1)
        columns = jnp.concatenate(
            [columns, jnp.zeros((HV - columns.shape[0], HV), F32)], axis=0
        )
        columns = jnp.transpose(columns)[:ROWS]
        for head in range(TP):
            g, j = head // GROUP, head % GROUP
            ratios = []
            for m in range(2):
                index = 2 * j + m
                ratio = jnp.zeros((ROWS, HV), F32)
                for t in range(g * GROUP, (g + 1) * GROUP):
                    part = parts_ref[t, index * ROWS : (index + 1) * ROWS, :].astype(F32)
                    column = t * STATS + index
                    ratio = ratio + columns[:, column : column + 1] * part
                ratios.append(ratio)
            column = TP * STATS + head
            attended = ratios[0] - columns[:, column : column + 1] * ratios[1]
            square = jnp.mean(attended * attended, axis=-1, keepdims=True)
            gate = parts_ref[head, GATE_ROW:STAT_ROW, :].astype(F32)
            branch = attended * lax.rsqrt(square + NORM_EPSILON) * head_gain_ref[...] * silu(gate)
            branch_ref[g, :, j * HV : (j + 1) * HV] = branch.astype(BF16)

    own = core_ref[0]
    pieces = own_ref.shape[0]
    for piece in range(pieces):
        projected = jnp.dot(branch_ref[own], own_ref[piece], preferred_element_type=F32)
        projected = projected + jnp.dot(
            branch_ref[1 - own], other_ref[piece], preferred_element_type=F32
        )
        projected_ref[step * pieces + piece] = projected.astype(BF16).astype(F32)

    @pl.when(step == pl.num_programs(0) - 1)
    def _():
        square = jnp.zeros((ROWS, 1), F32)
        for t in range(TP):
            square = square + jnp.sum(projected_ref[t] * projected_ref[t], axis=-1, keepdims=True)
        factor = lax.rsqrt(square / D + NORM_EPSILON)
        out_gate = vector_of(sums_ref, 2)
        gain = post_gain_ref[...]
        width = D // TP
        for t in range(TP):
            columns = slice(t * width, (t + 1) * width)
            value = projected_ref[t] * factor * gain[:, columns] * out_gate[:, columns]
            out_ref[:, columns] = value.astype(BF16)


def whole_block(shape):
    return pl.BlockSpec(shape, lambda *_: (0,) * len(shape))


def compute(
    latents, condition, context, context_cond, shift_weight, scale_weight, out_gate_weight,
    pre_gain, post_gain, query_weight, key_weight, value_weight, head_gate_weight,
    lambdas, head_gain, out_weight,
):
    params = pltpu.CompilerParams(vmem_limit_bytes=VMEM_LIMIT)
    both_axes = ("sp", "tp")
    t = lax.axis_index("tp")
    core = lax.axis_index("dp") % 2
    rows = lax.all_gather(latents[0], "tp", axis=0, tiled=False)
    other_context = lax.ppermute(
        context[0], "tp", [(i, (i + GROUP) % TP) for i in range(TP)]
    )
    partials = pl.pallas_call(
        partial_sums_kernel,
        out_shape=jax.ShapeDtypeStruct((SP * TP, 1, CHUNK), F32),
        compiler_params=params,
        name="partial_sums",
    )(condition, context_cond[None, :], shift_weight, scale_weight, out_gate_weight)
    pieces = lax.all_to_all(partials, both_axes, split_axis=0, concat_axis=0, tiled=True)
    own_sums = jnp.sum(pieces, axis=0, keepdims=True)
    copies = jnp.broadcast_to(own_sums, pieces.shape)
    sums = lax.all_to_all(copies, both_axes, split_axis=0, concat_axis=0, tiled=True)
    half = lax.dynamic_slice_in_dim(out_weight, core * GROUP * HV, GROUP * HV, 0)
    half = half + (own_sums[0, 0, 0] * 0.0).astype(BF16)
    own_half = lax.all_gather(half, "tp", axis=0, tiled=False)
    other_half = lax.ppermute(own_half, "dp", [(i, i ^ 1) for i in range(8)])
    place = jnp.stack([t % GROUP, t // GROUP]).astype(jnp.int32)
    queries, head_gate, key_values = pl.pallas_call(
        project_kernel,
        grid_spec=pltpu.PrefetchScalarGridSpec(
            num_scalar_prefetch=1,
            grid=(TP // 2,),
            in_specs=[
                pl.BlockSpec((2, ROWS, D), lambda i, _: (i, 0, 0)),
                whole_block((CTX_ROWS, D)),
                whole_block((CTX_ROWS, D)),
                whole_block((SP * TP, 1, CHUNK)),
                whole_block((1, D)),
                whole_block((D, HV)),
                whole_block((D, HV)),
                pl.BlockSpec((D, HV), lambda i, place_ref: (0, place_ref[1])),
                pl.BlockSpec((D, HV), lambda i, place_ref: (0, place_ref[1])),
            ],
            out_specs=[
                whole_block((GROUP, TP * ROWS, HV)),
                whole_block((TP * ROWS, HV)),
                whole_block((QUARTER, 2 * HV)),
            ],
            scratch_shapes=[pltpu.VMEM((TP * ROWS, D), BF16)],
        ),
        out_shape=[
            jax.ShapeDtypeStruct((GROUP, TP * ROWS, HV), BF16),
            jax.ShapeDtypeStruct((TP * ROWS, HV), BF16),
            jax.ShapeDtypeStruct((QUARTER, 2 * HV), BF16),
        ],
        compiler_params=params,
        name="project",
    )(
        place, rows, context[0], other_context, sums, pre_gain[None, :],
        query_weight, head_gate_weight, key_weight, value_weight,
    )
    key_values = lax.all_gather(key_values, "sp", axis=0, tiled=True)
    queries = lax.all_to_all(
        queries, "tp", split_axis=0, concat_axis=0, axis_index_groups=TP_GROUPS, tiled=True
    )
    peers = 4
    parts = pl.pallas_call(
        attention_kernel,
        grid=(TP // peers,),
        in_specs=[
            pl.BlockSpec(memory_space=pltpu.SMEM),
            pl.BlockSpec((GROUP, peers * ROWS, HV), lambda i: (0, i, 0)),
            whole_block((KEYS, 2 * HV)),
            pl.BlockSpec((peers * ROWS, HV), lambda i: (i, 0)),
        ],
        out_specs=pl.BlockSpec((peers, MESSAGE, HV), lambda i: (i, 0, 0)),
        out_shape=jax.ShapeDtypeStruct((TP, MESSAGE, HV), BF16),
        compiler_params=params,
        name="attention",
    )(lambdas, queries, key_values, head_gate)
    parts = lax.all_to_all(parts, "tp", split_axis=0, concat_axis=0, tiled=True)
    weight_block = pl.BlockSpec((2, GROUP * HV, D // TP), lambda i, _: (i, 0, 0))
    mixed_out = pl.pallas_call(
        finish_kernel,
        grid_spec=pltpu.PrefetchScalarGridSpec(
            num_scalar_prefetch=1,
            grid=(TP // 2,),
            in_specs=[
                whole_block((TP, MESSAGE, HV)),
                weight_block,
                weight_block,
                whole_block((SP * TP, 1, CHUNK)),
                whole_block((1, D)),
                whole_block((1, HV)),
            ],
            out_specs=whole_block((ROWS, D)),
            scratch_shapes=[
                pltpu.VMEM((2, ROWS, GROUP * HV), BF16),
                pltpu.VMEM((TP, ROWS, D // TP), F32),
            ],
        ),
        out_shape=jax.ShapeDtypeStruct((ROWS, D), BF16),
        compiler_params=params,
        name="finish",
    )(
        core.astype(jnp.int32)[None], parts, own_half, other_half, sums,
        post_gain[None, :], head_gain[None, :],
    )
    return mixed_out[None]


def solution(mesh):
    tokens = P("dp", ("sp", "tp"), None)
    channels = P(("sp", "tp"), None)
    return jax.shard_map(
        compute,
        mesh=mesh,
        in_specs=(
            tokens, P("dp", ("sp", "tp")), tokens, P(("sp", "tp")), channels, channels, channels,
            P(), P(), P(None, "tp"), P(), P(), P(None, "tp"), P("tp"), P(), P(None, "tp"),
        ),
        out_specs=tokens,
        check_vma=False,
    )
```

```python
import jax
import jax.numpy as jnp
from jax import lax
from jax.experimental import pallas as pl
from jax.experimental.pallas import tpu as pltpu
from jax.sharding import PartitionSpec as P


D = 3072
GROUP = 4
HQK = 64
HV = 128
ROWS = 64
CTX_ROWS = 4
TP = 8
SP = 12
QUARTER = 2 * (ROWS + CTX_ROWS)
KEYS = SP * QUARTER
STATS = GROUP * 2
GATE_ROW = STATS * ROWS
STAT_ROW = GATE_ROW + ROWS
MESSAGE = STAT_ROW + 2 * STATS
CHUNK = 256
CHAIN = 512
FINISH_PIECES = 4
PROJECT_PIECES = 4
VECTOR_ROWS = D // CHUNK
SCALE = HQK ** (-0.5) * 1.4426950408889634
NORM_EPSILON = 1e-06
F32 = jnp.float32
BF16 = jnp.bfloat16
TP_GROUPS = [[0, 1, 2, 3], [4, 5, 6, 7]]
CORE_PAIRS = [[0, 1], [2, 3], [4, 5], [6, 7]]
VMEM_LIMIT = 60 * 1024 * 1024


def silu(values):
    return values / (1.0 + jnp.exp(-values))


def partial_sums_kernel(cond_ref, ctx_ref, shift_ref, scale_ref, gate_ref, out_ref):
    both = jnp.concatenate([cond_ref[...], ctx_ref[...]], axis=0).astype(F32)
    both = silu(both).astype(BF16)
    out_ref[...] = jnp.zeros_like(out_ref)
    shift = jnp.dot(both, shift_ref[...], preferred_element_type=F32)
    scale = jnp.dot(both, scale_ref[...], preferred_element_type=F32)
    gate = jnp.dot(both, gate_ref[...], preferred_element_type=F32)
    vectors = [shift[:1], scale[:1], gate[:1], shift[1:], scale[1:]]
    for number, vector in enumerate(vectors):
        for piece in range(VECTOR_ROWS):
            row = number * VECTOR_ROWS + piece
            out_ref[row] = vector[:, piece * CHUNK : (piece + 1) * CHUNK]


def vector_of(sums_ref, number):
    first = number * VECTOR_ROWS
    return jnp.concatenate(
        [sums_ref[first + piece] for piece in range(VECTOR_ROWS)], axis=1
    )


def modulated(tokens, scale, shift):
    values = tokens.astype(F32)
    square = jnp.mean(values * values, axis=-1, keepdims=True)
    return (values * lax.rsqrt(square + NORM_EPSILON) * scale + shift).astype(BF16)


def project_kernel(
    place_ref, rows_ref, own_ref, other_ref, sums_ref, gain_ref,
    query_weight_ref, gate_weight_ref, key_weight_ref, value_weight_ref,
    q_ref, gate_ref, kv_ref, latent_ref,
):
    step = pl.program_id(0)
    pieces = rows_ref.shape[0]
    block = pieces * ROWS
    gain = gain_ref[...]
    scale, shift = gain * (1.0 + vector_of(sums_ref, 1)), vector_of(sums_ref, 0)
    latent = modulated(rows_ref[...].reshape(block, D), scale, shift)
    weight = jnp.concatenate([query_weight_ref[...], gate_weight_ref[...]], axis=1)
    projected = jnp.dot(latent, weight, preferred_element_type=F32).astype(BF16)
    first = pl.multiple_of(step * block, block)
    for copy in range(GROUP):
        q_ref[copy, pl.ds(first, block), :] = projected[:, :HV]
    gate_ref[pl.ds(first, block), :] = projected[:, HV:]
    quarter_step = place_ref[0] * 2 // pieces

    @pl.when(step == quarter_step)
    def _():
        weight = jnp.concatenate([key_weight_ref[...], value_weight_ref[...]], axis=1)
        context = jnp.concatenate([own_ref[...].astype(F32), other_ref[...].astype(F32)], axis=0)
        context_scale = gain * (1.0 + vector_of(sums_ref, 4))
        context = modulated(context, context_scale, vector_of(sums_ref, 3))
        latent_ref[...] = latent
        inner = pl.multiple_of((place_ref[0] * 2 - quarter_step * pieces) * ROWS, 2 * ROWS)
        tokens = jnp.concatenate([latent_ref[pl.ds(inner, 2 * ROWS), :], context], axis=0)
        kv_ref[...] = jnp.dot(tokens, weight, preferred_element_type=F32).astype(BF16)


def three_parts(value):
    high = value.astype(BF16)
    rest = value - high.astype(F32)
    middle = rest.astype(BF16)
    low = (rest - middle.astype(F32)).astype(BF16)
    return high.astype(F32), middle.astype(F32), low.astype(F32)


def attention_kernel(lambda_ref, q_ref, kv_ref, gate_ref, out_ref):
    peers = out_ref.shape[0]
    block = peers * ROWS
    q = q_ref[...].reshape(GROUP * block, 2 * HQK)
    keys = kv_ref[:, : 2 * HQK]
    value_rows = kv_ref[:, 2 * HQK :]
    lane = lax.broadcasted_iota(jnp.int32, (CHAIN, 2 * HQK), 1)
    chains = [(first, m) for first in range(0, GROUP * block, CHAIN) for m in range(2)]

    def scores_of(first, m):
        rows = q[first : first + CHAIN]
        rows = jnp.where(lane // HQK == m, rows, jnp.zeros_like(rows))
        return lax.dot_general(rows, keys, (((1,), (1,)), ((), ())), preferred_element_type=F32)

    def exponent_of(scores):
        largest = jnp.max(scores, axis=-1, keepdims=True) * SCALE
        exponent = jnp.exp2(scores * SCALE - largest)
        return exponent.astype(BF16), jnp.sum(exponent, axis=-1, keepdims=True), largest

    def ratio_of(weights, total, largest):
        weighted = jnp.dot(weights, value_rows, preferred_element_type=F32)
        return (weighted / total).astype(BF16), largest + jnp.log2(total)

    ahead, waiting, ratios, levels = scores_of(*chains[0]), None, {}, {}

    def settle():
        first, m = waiting[0]
        ratio, level = ratio_of(*waiting[1])
        for inner in range(0, CHAIN, block):
            head = (first + inner) // block
            ratios[head, m] = ratio[inner : inner + block]
            levels[head, m] = level[inner : inner + block]

    for number, chain in enumerate(chains):
        scores = ahead
        if number + 1 < len(chains):
            ahead = scores_of(*chains[number + 1])
        exponent = exponent_of(scores)
        if waiting is not None:
            settle()
        waiting = (chain, exponent)
    settle()

    stat_lane = lax.broadcasted_iota(jnp.int32, (block, HV), 1)
    stats = jnp.zeros((block, HV), F32)
    for (head, m), ratio in ratios.items():
        index = 2 * head + m
        for p in range(peers):
            out_ref[p, index * ROWS : (index + 1) * ROWS, :] = ratio[p * ROWS : (p + 1) * ROWS]
        wide = jnp.broadcast_to(levels[head, m], (block, HV))
        stats = jnp.where(stat_lane == index, wide, stats)
    high, middle, low = three_parts(jnp.transpose(stats)[:STATS])
    row = lax.broadcasted_iota(jnp.int32, (STATS, ROWS), 0)
    own_lambda = jnp.zeros((STATS, ROWS), F32)
    for part, piece in enumerate(three_parts(jnp.full((STATS, ROWS), lambda_ref[0], F32))):
        own_lambda = jnp.where(row == part, piece, own_lambda)
    for p in range(peers):
        lanes = slice(p * ROWS, (p + 1) * ROWS)
        out_ref[p, GATE_ROW:STAT_ROW, :] = gate_ref[lanes, :]
        upper = jnp.concatenate([high[:, lanes], middle[:, lanes]], axis=1)
        lower = jnp.concatenate([low[:, lanes], own_lambda], axis=1)
        out_ref[p, STAT_ROW:, :] = jnp.concatenate([upper, lower], axis=0).astype(BF16)


def finish_kernel(
    parts_ref, weight_ref, sums_ref, post_gain_ref, head_gain_ref, out_ref, branch_ref, projected_ref
):
    step = pl.program_id(0)

    @pl.when(step == 0)
    def _():
        levels, lambdas = [], []
        for t in range(TP):
            stats = parts_ref[t, STAT_ROW:, :].astype(F32)
            upper, lower = stats[:STATS], stats[STATS:]
            levels.append(upper[:, :ROWS] + upper[:, ROWS:] + lower[:, :ROWS])
            lambdas.append(lower[0:1, ROWS:] + lower[1:2, ROWS:] + lower[2:3, ROWS:])
        shares = []
        for g in range(TP // GROUP):
            group = levels[g * GROUP : (g + 1) * GROUP]
            top = jnp.maximum(jnp.maximum(group[0], group[1]), jnp.maximum(group[2], group[3]))
            group = [jnp.exp2(level - top) for level in group]
            total = group[0] + group[1] + group[2] + group[3]
            shares = shares + [share / total for share in group]
        columns = jnp.concatenate(shares + lambdas, axis=0)
        columns = jnp.concatenate([columns, jnp.zeros_like(columns)], axis=1)
        columns = jnp.concatenate(
            [columns, jnp.zeros((HV - columns.shape[0], HV), F32)], axis=0
        )
        columns = jnp.transpose(columns)[:ROWS]
        for head in range(TP):
            g, j = head // GROUP, head % GROUP
            ratios = []
            for m in range(2):
                index = 2 * j + m
                ratio = jnp.zeros((ROWS, HV), F32)
                for t in range(g * GROUP, (g + 1) * GROUP):
                    part = parts_ref[t, index * ROWS : (index + 1) * ROWS, :].astype(F32)
                    column = t * STATS + index
                    ratio = ratio + columns[:, column : column + 1] * part
                ratios.append(ratio)
            column = TP * STATS + head
            attended = ratios[0] - columns[:, column : column + 1] * ratios[1]
            square = jnp.mean(attended * attended, axis=-1, keepdims=True)
            gate = parts_ref[head, GATE_ROW:STAT_ROW, :].astype(F32)
            branch = attended * lax.rsqrt(square + NORM_EPSILON) * head_gain_ref[...] * silu(gate)
            branch_ref[:, head * HV : (head + 1) * HV] = branch.astype(BF16)

    pieces = weight_ref.shape[1]
    for piece in range(pieces):
        weight = weight_ref[:, piece].reshape(TP * HV, D // TP)
        projected = jnp.dot(branch_ref[...], weight, preferred_element_type=F32)
        projected_ref[step * pieces + piece] = projected.astype(BF16).astype(F32)

    @pl.when(step == pl.num_programs(0) - 1)
    def _():
        square = jnp.zeros((ROWS, 1), F32)
        for t in range(TP):
            square = square + jnp.sum(projected_ref[t] * projected_ref[t], axis=-1, keepdims=True)
        factor = lax.rsqrt(square / D + NORM_EPSILON)
        out_gate = vector_of(sums_ref, 2)
        gain = post_gain_ref[...]
        width = D // TP
        for t in range(TP):
            columns = slice(t * width, (t + 1) * width)
            value = projected_ref[t] * factor * gain[:, columns] * out_gate[:, columns]
            out_ref[:, columns] = value.astype(BF16)


def whole_block(shape):
    return pl.BlockSpec(shape, lambda *_: (0,) * len(shape))


def compute(
    latents, condition, context, context_cond, shift_weight, scale_weight, out_gate_weight,
    pre_gain, post_gain, query_weight, key_weight, value_weight, head_gate_weight,
    lambdas, head_gain, out_weight,
):
    params = pltpu.CompilerParams(vmem_limit_bytes=VMEM_LIMIT)
    both_axes = ("sp", "tp")
    t = lax.axis_index("tp")
    core = lax.axis_index("dp") % 2
    rows = lax.all_gather(latents[0], "tp", axis=0, tiled=False)
    other_context = lax.ppermute(
        context[0], "tp", [(i, (i + GROUP) % TP) for i in range(TP)]
    )
    partials = pl.pallas_call(
        partial_sums_kernel,
        out_shape=jax.ShapeDtypeStruct((SP * TP, 1, CHUNK), F32),
        compiler_params=params,
        name="partial_sums",
    )(condition, context_cond[None, :], shift_weight, scale_weight, out_gate_weight)
    pieces = lax.all_to_all(partials, both_axes, split_axis=0, concat_axis=0, tiled=True)
    own_sums = jnp.sum(pieces, axis=0, keepdims=True)
    copies = jnp.broadcast_to(own_sums, pieces.shape)
    sums = lax.all_to_all(copies, both_axes, split_axis=0, concat_axis=0, tiled=True)
    half = lax.dynamic_slice_in_dim(out_weight, core * GROUP * HV, GROUP * HV, 0)
    half = half + (own_sums[0, 0, 0] * 0.0).astype(BF16)
    halves = lax.all_gather(half, "tp", axis=0, tiled=False)
    out_weights = lax.all_gather(halves, "dp", axis=0, tiled=False, axis_index_groups=CORE_PAIRS)
    place = jnp.stack([t % GROUP, t // GROUP]).astype(jnp.int32)
    queries, head_gate, key_values = pl.pallas_call(
        project_kernel,
        grid_spec=pltpu.PrefetchScalarGridSpec(
            num_scalar_prefetch=1,
            grid=(TP // PROJECT_PIECES,),
            in_specs=[
                pl.BlockSpec((PROJECT_PIECES, ROWS, D), lambda i, _: (i, 0, 0)),
                whole_block((CTX_ROWS, D)),
                whole_block((CTX_ROWS, D)),
                whole_block((SP * TP, 1, CHUNK)),
                whole_block((1, D)),
                whole_block((D, HV)),
                whole_block((D, HV)),
                pl.BlockSpec((D, HV), lambda i, place_ref: (0, place_ref[1])),
                pl.BlockSpec((D, HV), lambda i, place_ref: (0, place_ref[1])),
            ],
            out_specs=[
                whole_block((GROUP, TP * ROWS, HV)),
                whole_block((TP * ROWS, HV)),
                whole_block((QUARTER, 2 * HV)),
            ],
            scratch_shapes=[pltpu.VMEM((PROJECT_PIECES * ROWS, D), BF16)],
        ),
        out_shape=[
            jax.ShapeDtypeStruct((GROUP, TP * ROWS, HV), BF16),
            jax.ShapeDtypeStruct((TP * ROWS, HV), BF16),
            jax.ShapeDtypeStruct((QUARTER, 2 * HV), BF16),
        ],
        compiler_params=params,
        name="project",
    )(
        place, rows, context[0], other_context, sums, pre_gain[None, :],
        query_weight, head_gate_weight, key_weight, value_weight,
    )
    key_values = lax.all_gather(key_values, "sp", axis=0, tiled=True)
    queries = lax.all_to_all(
        queries, "tp", split_axis=0, concat_axis=0, axis_index_groups=TP_GROUPS, tiled=True
    )
    peers = 4
    parts = pl.pallas_call(
        attention_kernel,
        grid=(TP // peers,),
        in_specs=[
            pl.BlockSpec(memory_space=pltpu.SMEM),
            pl.BlockSpec((GROUP, peers * ROWS, HV), lambda i: (0, i, 0)),
            whole_block((KEYS, 2 * HV)),
            pl.BlockSpec((peers * ROWS, HV), lambda i: (i, 0)),
        ],
        out_specs=pl.BlockSpec((peers, MESSAGE, HV), lambda i: (i, 0, 0)),
        out_shape=jax.ShapeDtypeStruct((TP, MESSAGE, HV), BF16),
        compiler_params=params,
        name="attention",
    )(lambdas, queries, key_values, head_gate)
    parts = lax.all_to_all(parts, "tp", split_axis=0, concat_axis=0, tiled=True)
    mixed_out = pl.pallas_call(
        finish_kernel,
        grid=(TP // FINISH_PIECES,),
        in_specs=[
            whole_block((TP, MESSAGE, HV)),
            pl.BlockSpec((2, FINISH_PIECES, GROUP * HV, D // TP), lambda i: (0, i, 0, 0)),
            whole_block((SP * TP, 1, CHUNK)),
            whole_block((1, D)),
            whole_block((1, HV)),
        ],
        out_specs=whole_block((ROWS, D)),
        out_shape=jax.ShapeDtypeStruct((ROWS, D), BF16),
        scratch_shapes=[pltpu.VMEM((ROWS, TP * HV), BF16), pltpu.VMEM((TP, ROWS, D // TP), F32)],
        compiler_params=params,
        name="finish",
    )(parts, out_weights, sums, post_gain[None, :], head_gain[None, :])
    return mixed_out[None]


def solution(mesh):
    tokens = P("dp", ("sp", "tp"), None)
    channels = P(("sp", "tp"), None)
    return jax.shard_map(
        compute,
        mesh=mesh,
        in_specs=(
            tokens, P("dp", ("sp", "tp")), tokens, P(("sp", "tp")), channels, channels, channels,
            P(), P(), P(None, "tp"), P(), P(), P(None, "tp"), P("tp"), P(), P(None, "tp"),
        ),
        out_specs=tokens,
        check_vma=False,
    )
```

```python
import functools

import jax
import jax.numpy as jnp
from jax import lax
from jax.experimental import pallas as pl
from jax.experimental.pallas import tpu as pltpu
from jax.sharding import PartitionSpec as P


D = 3072
GROUP = 4
HQK = 64
HV = 128
ROWS = 64
CTX_ROWS = 4
TP = 8
SP = 12
QUARTER = 2 * (ROWS + CTX_ROWS)
KEYS = SP * QUARTER
STATS = 8
PARTS = GROUP
GATE_ROW = PARTS * ROWS
CHUNK = 256
CHAIN = 512
PEERS = 8
FINISH_PIECES = 4
PROJECT_PIECES = 4
VECTOR_ROWS = D // CHUNK
SCALE = HQK ** (-0.5) * 1.4426950408889634
NORM_EPSILON = 1e-06
F32 = jnp.float32
BF16 = jnp.bfloat16
TP_GROUPS = [[0, 1, 2, 3], [4, 5, 6, 7]]
CORE_PAIRS = [[0, 1], [2, 3], [4, 5], [6, 7]]
VMEM_LIMIT = 60 * 1024 * 1024


def silu(values):
    return values / (1.0 + jnp.exp(-values))


def partial_sums_kernel(cond_ref, ctx_ref, shift_ref, scale_ref, gate_ref, out_ref):
    both = jnp.concatenate([cond_ref[...], ctx_ref[...]], axis=0).astype(F32)
    both = silu(both).astype(BF16)
    out_ref[...] = jnp.zeros_like(out_ref)
    shift = jnp.dot(both, shift_ref[...], preferred_element_type=F32)
    scale = jnp.dot(both, scale_ref[...], preferred_element_type=F32)
    gate = jnp.dot(both, gate_ref[...], preferred_element_type=F32)
    vectors = [shift[:1], scale[:1], gate[:1], shift[1:], scale[1:]]
    for number, vector in enumerate(vectors):
        for piece in range(VECTOR_ROWS):
            row = number * VECTOR_ROWS + piece
            out_ref[row] = vector[:, piece * CHUNK : (piece + 1) * CHUNK]


def vector_of(sums_ref, number):
    first = number * VECTOR_ROWS
    return jnp.concatenate(
        [sums_ref[first + piece] for piece in range(VECTOR_ROWS)], axis=1
    )


def modulated(tokens, scale, shift):
    values = tokens.astype(F32)
    square = jnp.mean(values * values, axis=-1, keepdims=True)
    return (values * lax.rsqrt(square + NORM_EPSILON) * scale + shift).astype(BF16)


def project_kernel(
    place_ref, rows_ref, own_ref, other_ref, sums_ref, gain_ref,
    query_weight_ref, gate_weight_ref, key_weight_ref, value_weight_ref,
    q_ref, gate_ref, kv_ref, latent_ref,
):
    step = pl.program_id(0)
    pieces = rows_ref.shape[0]
    block = pieces * ROWS
    gain = gain_ref[...]
    scale, shift = gain * (1.0 + vector_of(sums_ref, 1)), vector_of(sums_ref, 0)
    latent = modulated(rows_ref[...].reshape(block, D), scale, shift)
    weight = jnp.concatenate([query_weight_ref[...], gate_weight_ref[...]], axis=1)
    projected = jnp.dot(latent, weight, preferred_element_type=F32).astype(BF16)
    first = pl.multiple_of(step * block, block)
    for copy in range(GROUP):
        q_ref[copy, pl.ds(first, block), :] = projected[:, :HV]
    gate_ref[pl.ds(first, block), :] = projected[:, HV:]
    quarter_step = place_ref[0] * 2 // pieces

    @pl.when(step == quarter_step)
    def _():
        weight = jnp.concatenate([key_weight_ref[...], value_weight_ref[...]], axis=1)
        context = jnp.concatenate([own_ref[...].astype(F32), other_ref[...].astype(F32)], axis=0)
        context_scale = gain * (1.0 + vector_of(sums_ref, 4))
        context = modulated(context, context_scale, vector_of(sums_ref, 3))
        latent_ref[...] = latent
        inner = pl.multiple_of((place_ref[0] * 2 - quarter_step * pieces) * ROWS, 2 * ROWS)
        tokens = jnp.concatenate([latent_ref[pl.ds(inner, 2 * ROWS), :], context], axis=0)
        kv_ref[...] = jnp.dot(tokens, weight, preferred_element_type=F32).astype(BF16)


def three_parts(value):
    high = value.astype(BF16)
    rest = value - high.astype(F32)
    middle = rest.astype(BF16)
    low = (rest - middle.astype(F32)).astype(BF16)
    return high.astype(F32), middle.astype(F32), low.astype(F32)


def attention_kernel(with_gate, *refs):
    if with_gate:
        lambda_ref, gate_ref, q_ref, kv_ref, out_ref = refs
    else:
        q_ref, kv_ref, out_ref = refs
    peers = out_ref.shape[0]
    block = peers * ROWS
    q = q_ref[...].reshape(q_ref.shape[0] * block, 2 * HQK)
    keys = kv_ref[:, : 2 * HQK]
    value_rows = kv_ref[:, 2 * HQK :]
    lane = lax.broadcasted_iota(jnp.int32, (CHAIN, 2 * HQK), 1)
    chains = [(first, m) for first in range(0, q.shape[0], CHAIN) for m in range(2)]

    def scores_of(first, m):
        rows = q[first : first + CHAIN]
        rows = jnp.where(lane // HQK == m, rows, jnp.zeros_like(rows))
        return lax.dot_general(rows, keys, (((1,), (1,)), ((), ())), preferred_element_type=F32)

    def exponent_of(scores):
        largest = jnp.max(scores, axis=-1, keepdims=True) * SCALE
        exponent = jnp.exp2(scores * SCALE - largest)
        return exponent.astype(BF16), jnp.sum(exponent, axis=-1, keepdims=True), largest

    def ratio_of(weights, total, largest):
        weighted = jnp.dot(weights, value_rows, preferred_element_type=F32)
        return (weighted / total).astype(BF16), largest + jnp.log2(total)

    ahead, waiting, ratios, levels = scores_of(*chains[0]), None, {}, {}

    def settle():
        first, m = waiting[0]
        ratio, level = ratio_of(*waiting[1])
        for inner in range(0, CHAIN, block):
            head = (first + inner) // block
            ratios[head, m] = ratio[inner : inner + block]
            levels[head, m] = level[inner : inner + block]

    for number, chain in enumerate(chains):
        scores = ahead
        if number + 1 < len(chains):
            ahead = scores_of(*chains[number + 1])
        exponent = exponent_of(scores)
        if waiting is not None:
            settle()
        waiting = (chain, exponent)
    settle()

    stat_lane = lax.broadcasted_iota(jnp.int32, (block, HV), 1)
    stats = jnp.zeros((block, HV), F32)
    for (head, m), ratio in ratios.items():
        index = 2 * head + m
        for p in range(peers):
            out_ref[p, index * ROWS : (index + 1) * ROWS, :] = ratio[p * ROWS : (p + 1) * ROWS]
        wide = jnp.broadcast_to(levels[head, m], (block, HV))
        stats = jnp.where(stat_lane == index, wide, stats)
    high, middle, low = three_parts(jnp.transpose(stats)[:STATS])
    row = lax.broadcasted_iota(jnp.int32, (STATS, ROWS), 0)
    own_lambda = jnp.zeros((STATS, ROWS), F32)
    if with_gate:
        for part, piece in enumerate(three_parts(jnp.full((STATS, ROWS), lambda_ref[0], F32))):
            own_lambda = jnp.where(row == part, piece, own_lambda)
    stat_row = out_ref.shape[1] - 2 * STATS
    for p in range(peers):
        lanes = slice(p * ROWS, (p + 1) * ROWS)
        if with_gate:
            out_ref[p, GATE_ROW:stat_row, :] = gate_ref[lanes, :]
        upper = jnp.concatenate([high[:, lanes], middle[:, lanes]], axis=1)
        lower = jnp.concatenate([low[:, lanes], own_lambda], axis=1)
        out_ref[p, stat_row:, :] = jnp.concatenate([upper, lower], axis=0).astype(BF16)


def finish_kernel(
    first_ref, second_ref, weight_ref, sums_ref, post_gain_ref, head_gain_ref,
    out_ref, branch_ref, projected_ref,
):
    step = pl.program_id(0)

    @pl.when(step == 0)
    def _():
        levels, lambdas = [], []
        for t in range(TP):
            both = []
            for parts_ref in (first_ref, second_ref):
                stats = parts_ref[t, parts_ref.shape[1] - 2 * STATS :, :].astype(F32)
                upper, lower = stats[:STATS], stats[STATS:]
                level = upper[:, :ROWS] + upper[:, ROWS:] + lower[:, :ROWS]
                both.append(level[:PARTS])
                if parts_ref is first_ref:
                    lambdas.append(lower[0:1, ROWS:] + lower[1:2, ROWS:] + lower[2:3, ROWS:])
            levels.append(jnp.concatenate(both, axis=0))
        shares = []
        for g in range(TP // GROUP):
            group = levels[g * GROUP : (g + 1) * GROUP]
            top = jnp.maximum(jnp.maximum(group[0], group[1]), jnp.maximum(group[2], group[3]))
            group = [jnp.exp2(level - top) for level in group]
            total = group[0] + group[1] + group[2] + group[3]
            shares = shares + [share / total for share in group]
        columns = jnp.concatenate(shares + lambdas, axis=0)
        columns = jnp.concatenate([columns, jnp.zeros_like(columns)], axis=1)
        columns = jnp.concatenate(
            [columns, jnp.zeros((HV - columns.shape[0], HV), F32)], axis=0
        )
        columns = jnp.transpose(columns)[:ROWS]
        for head in range(TP):
            g, j = head // GROUP, head % GROUP
            ratios = []
            for m in range(2):
                index = 2 * j + m
                ratio = jnp.zeros((ROWS, HV), F32)
                parts_ref = first_ref if index < PARTS else second_ref
                first = index % PARTS * ROWS
                for t in range(g * GROUP, (g + 1) * GROUP):
                    part = parts_ref[t, first : first + ROWS, :].astype(F32)
                    column = t * STATS + index
                    ratio = ratio + columns[:, column : column + 1] * part
                ratios.append(ratio)
            column = TP * STATS + head
            attended = ratios[0] - columns[:, column : column + 1] * ratios[1]
            square = jnp.mean(attended * attended, axis=-1, keepdims=True)
            gate = first_ref[head, GATE_ROW : GATE_ROW + ROWS, :].astype(F32)
            branch = attended * lax.rsqrt(square + NORM_EPSILON) * head_gain_ref[...] * silu(gate)
            branch_ref[:, head * HV : (head + 1) * HV] = branch.astype(BF16)

    pieces = weight_ref.shape[1]
    for piece in range(pieces):
        weight = weight_ref[:, piece].reshape(TP * HV, D // TP)
        projected = jnp.dot(branch_ref[...], weight, preferred_element_type=F32)
        projected_ref[step * pieces + piece] = projected.astype(BF16).astype(F32)

    @pl.when(step == pl.num_programs(0) - 1)
    def _():
        square = jnp.zeros((ROWS, 1), F32)
        for t in range(TP):
            square = square + jnp.sum(projected_ref[t] * projected_ref[t], axis=-1, keepdims=True)
        factor = lax.rsqrt(square / D + NORM_EPSILON)
        out_gate = vector_of(sums_ref, 2)
        gain = post_gain_ref[...]
        width = D // TP
        for t in range(TP):
            columns = slice(t * width, (t + 1) * width)
            value = projected_ref[t] * factor * gain[:, columns] * out_gate[:, columns]
            out_ref[:, columns] = value.astype(BF16)


def whole_block(shape):
    return pl.BlockSpec(shape, lambda *_: (0,) * len(shape))


def attend(queries, key_values, half, params, extra):
    rows = GATE_ROW + (ROWS if extra else 0) + 2 * STATS
    extra_specs = [
        pl.BlockSpec(memory_space=pltpu.SMEM), pl.BlockSpec((PEERS * ROWS, HV), lambda i: (i, 0))
    ]
    return pl.pallas_call(
        functools.partial(attention_kernel, bool(extra)),
        grid=(TP // PEERS,),
        in_specs=(extra_specs if extra else [])
        + [
            pl.BlockSpec((GROUP // 2, PEERS * ROWS, HV), lambda i: (half, i, 0)),
            whole_block((KEYS, 2 * HV)),
        ],
        out_specs=pl.BlockSpec((PEERS, rows, HV), lambda i: (i, 0, 0)),
        out_shape=jax.ShapeDtypeStruct((TP, rows, HV), BF16),
        compiler_params=params,
        name="attention",
    )(*extra, queries, key_values)


def compute(
    latents, condition, context, context_cond, shift_weight, scale_weight, out_gate_weight,
    pre_gain, post_gain, query_weight, key_weight, value_weight, head_gate_weight,
    lambdas, head_gain, out_weight,
):
    params = pltpu.CompilerParams(vmem_limit_bytes=VMEM_LIMIT)
    both_axes = ("sp", "tp")
    t = lax.axis_index("tp")
    core = lax.axis_index("dp") % 2
    rows = lax.all_gather(latents[0], "tp", axis=0, tiled=False)
    other_context = lax.ppermute(
        context[0], "tp", [(i, (i + GROUP) % TP) for i in range(TP)]
    )
    partials = pl.pallas_call(
        partial_sums_kernel,
        out_shape=jax.ShapeDtypeStruct((SP * TP, 1, CHUNK), F32),
        compiler_params=params,
        name="partial_sums",
    )(condition, context_cond[None, :], shift_weight, scale_weight, out_gate_weight)
    pieces = lax.all_to_all(partials, both_axes, split_axis=0, concat_axis=0, tiled=True)
    own_sums = jnp.sum(pieces, axis=0, keepdims=True)
    copies = jnp.broadcast_to(own_sums, pieces.shape)
    sums = lax.all_to_all(copies, both_axes, split_axis=0, concat_axis=0, tiled=True)
    half = lax.dynamic_slice_in_dim(out_weight, core * GROUP * HV, GROUP * HV, 0)
    half = half + (own_sums[0, 0, 0] * 0.0).astype(BF16)
    halves = lax.all_gather(half, "tp", axis=0, tiled=False)
    out_weights = lax.all_gather(halves, "dp", axis=0, tiled=False, axis_index_groups=CORE_PAIRS)
    place = jnp.stack([t % GROUP, t // GROUP]).astype(jnp.int32)
    queries, head_gate, key_values = pl.pallas_call(
        project_kernel,
        grid_spec=pltpu.PrefetchScalarGridSpec(
            num_scalar_prefetch=1,
            grid=(TP // PROJECT_PIECES,),
            in_specs=[
                pl.BlockSpec((PROJECT_PIECES, ROWS, D), lambda i, _: (i, 0, 0)),
                whole_block((CTX_ROWS, D)),
                whole_block((CTX_ROWS, D)),
                whole_block((SP * TP, 1, CHUNK)),
                whole_block((1, D)),
                whole_block((D, HV)),
                whole_block((D, HV)),
                pl.BlockSpec((D, HV), lambda i, place_ref: (0, place_ref[1])),
                pl.BlockSpec((D, HV), lambda i, place_ref: (0, place_ref[1])),
            ],
            out_specs=[
                whole_block((GROUP, TP * ROWS, HV)),
                whole_block((TP * ROWS, HV)),
                whole_block((QUARTER, 2 * HV)),
            ],
            scratch_shapes=[pltpu.VMEM((PROJECT_PIECES * ROWS, D), BF16)],
        ),
        out_shape=[
            jax.ShapeDtypeStruct((GROUP, TP * ROWS, HV), BF16),
            jax.ShapeDtypeStruct((TP * ROWS, HV), BF16),
            jax.ShapeDtypeStruct((QUARTER, 2 * HV), BF16),
        ],
        compiler_params=params,
        name="project",
    )(
        place, rows, context[0], other_context, sums, pre_gain[None, :],
        query_weight, head_gate_weight, key_weight, value_weight,
    )
    key_values = lax.all_gather(key_values, "sp", axis=0, tiled=True)
    queries = lax.all_to_all(
        queries, "tp", split_axis=0, concat_axis=0, axis_index_groups=TP_GROUPS, tiled=True
    )
    first_parts = attend(queries, key_values, 0, params, (lambdas, head_gate))
    first_parts = lax.all_to_all(first_parts, "tp", split_axis=0, concat_axis=0, tiled=True)
    second_parts = attend(queries, key_values, 1, params, ())
    second_parts = lax.all_to_all(second_parts, "tp", split_axis=0, concat_axis=0, tiled=True)
    mixed_out = pl.pallas_call(
        finish_kernel,
        grid=(TP // FINISH_PIECES,),
        in_specs=[
            whole_block(first_parts.shape),
            whole_block(second_parts.shape),
            pl.BlockSpec((2, FINISH_PIECES, GROUP * HV, D // TP), lambda i: (0, i, 0, 0)),
            whole_block((SP * TP, 1, CHUNK)),
            whole_block((1, D)),
            whole_block((1, HV)),
        ],
        out_specs=whole_block((ROWS, D)),
        out_shape=jax.ShapeDtypeStruct((ROWS, D), BF16),
        scratch_shapes=[pltpu.VMEM((ROWS, TP * HV), BF16), pltpu.VMEM((TP, ROWS, D // TP), F32)],
        compiler_params=params,
        name="finish",
    )(first_parts, second_parts, out_weights, sums, post_gain[None, :], head_gain[None, :])
    return mixed_out[None]


def solution(mesh):
    tokens = P("dp", ("sp", "tp"), None)
    channels = P(("sp", "tp"), None)
    return jax.shard_map(
        compute,
        mesh=mesh,
        in_specs=(
            tokens, P("dp", ("sp", "tp")), tokens, P(("sp", "tp")), channels, channels, channels,
            P(), P(), P(None, "tp"), P(), P(), P(None, "tp"), P("tp"), P(), P(None, "tp"),
        ),
        out_specs=tokens,
        check_vma=False,
    )
```

```python
import functools

import jax
import jax.numpy as jnp
from jax import lax
from jax.experimental import pallas as pl
from jax.experimental.pallas import tpu as pltpu
from jax.sharding import PartitionSpec as P


D = 3072
GROUP = 4
HQK = 64
HV = 128
ROWS = 64
CTX_ROWS = 4
TP = 8
SP = 12
QUARTER = 2 * (ROWS + CTX_ROWS)
KEYS = SP * QUARTER
STATS = 8
PARTS = GROUP
GATE_ROW = PARTS * ROWS
CHUNK = 256
CHAIN = 512
PEERS = 8
FINISH_PIECES = 4
PROJECT_PIECES = 4
VECTOR_ROWS = D // CHUNK
SCALE = HQK ** (-0.5) * 1.4426950408889634
NORM_EPSILON = 1e-06
F32 = jnp.float32
BF16 = jnp.bfloat16
TP_GROUPS = [[0, 1, 2, 3], [4, 5, 6, 7]]
VMEM_LIMIT = 60 * 1024 * 1024


def silu(values):
    return values / (1.0 + jnp.exp(-values))


def partial_sums_kernel(cond_ref, ctx_ref, shift_ref, scale_ref, gate_ref, out_ref):
    both = jnp.concatenate([cond_ref[...], ctx_ref[...]], axis=0).astype(F32)
    both = silu(both).astype(BF16)
    out_ref[...] = jnp.zeros_like(out_ref)
    shift = jnp.dot(both, shift_ref[...], preferred_element_type=F32)
    scale = jnp.dot(both, scale_ref[...], preferred_element_type=F32)
    gate = jnp.dot(both, gate_ref[...], preferred_element_type=F32)
    vectors = [shift[:1], scale[:1], gate[:1], shift[1:], scale[1:]]
    for number, vector in enumerate(vectors):
        for piece in range(VECTOR_ROWS):
            row = number * VECTOR_ROWS + piece
            out_ref[row] = vector[:, piece * CHUNK : (piece + 1) * CHUNK]


def vector_of(sums_ref, number):
    first = number * VECTOR_ROWS
    return jnp.concatenate(
        [sums_ref[first + piece] for piece in range(VECTOR_ROWS)], axis=1
    )


def modulated(tokens, scale, shift):
    values = tokens.astype(F32)
    square = jnp.mean(values * values, axis=-1, keepdims=True)
    return (values * lax.rsqrt(square + NORM_EPSILON) * scale + shift).astype(BF16)


def project_kernel(
    place_ref, rows_ref, own_ref, other_ref, sums_ref, gain_ref,
    query_weight_ref, gate_weight_ref, key_weight_ref, value_weight_ref,
    q_ref, gate_ref, kv_ref, latent_ref,
):
    step = pl.program_id(0)
    pieces = rows_ref.shape[0]
    block = pieces * ROWS
    gain = gain_ref[...]
    scale, shift = gain * (1.0 + vector_of(sums_ref, 1)), vector_of(sums_ref, 0)
    latent = modulated(rows_ref[...].reshape(block, D), scale, shift)
    weight = jnp.concatenate([query_weight_ref[...], gate_weight_ref[...]], axis=1)
    projected = jnp.dot(latent, weight, preferred_element_type=F32).astype(BF16)
    first = pl.multiple_of(step * block, block)
    for copy in range(GROUP):
        q_ref[copy, pl.ds(first, block), :] = projected[:, :HV]
    gate_ref[pl.ds(first, block), :] = projected[:, HV:]
    quarter_step = place_ref[0] * 2 // pieces

    @pl.when(step == quarter_step)
    def _():
        weight = jnp.concatenate([key_weight_ref[...], value_weight_ref[...]], axis=1)
        context = jnp.concatenate([own_ref[...].astype(F32), other_ref[...].astype(F32)], axis=0)
        context_scale = gain * (1.0 + vector_of(sums_ref, 4))
        context = modulated(context, context_scale, vector_of(sums_ref, 3))
        latent_ref[...] = latent
        inner = pl.multiple_of((place_ref[0] * 2 - quarter_step * pieces) * ROWS, 2 * ROWS)
        tokens = jnp.concatenate([latent_ref[pl.ds(inner, 2 * ROWS), :], context], axis=0)
        kv_ref[...] = jnp.dot(tokens, weight, preferred_element_type=F32).astype(BF16)


def three_parts(value):
    high = value.astype(BF16)
    rest = value - high.astype(F32)
    middle = rest.astype(BF16)
    low = (rest - middle.astype(F32)).astype(BF16)
    return high.astype(F32), middle.astype(F32), low.astype(F32)


def attention_kernel(with_gate, *refs):
    if with_gate:
        lambda_ref, gate_ref, q_ref, kv_ref, out_ref = refs
    else:
        q_ref, kv_ref, out_ref = refs
    peers = out_ref.shape[0]
    block = peers * ROWS
    q = q_ref[...].reshape(q_ref.shape[0] * block, 2 * HQK)
    keys = kv_ref[:, : 2 * HQK]
    value_rows = kv_ref[:, 2 * HQK :]
    lane = lax.broadcasted_iota(jnp.int32, (CHAIN, 2 * HQK), 1)
    chains = [(first, m) for first in range(0, q.shape[0], CHAIN) for m in range(2)]

    def scores_of(first, m):
        rows = q[first : first + CHAIN]
        rows = jnp.where(lane // HQK == m, rows, jnp.zeros_like(rows))
        return lax.dot_general(rows, keys, (((1,), (1,)), ((), ())), preferred_element_type=F32)

    def exponent_of(scores):
        largest = jnp.max(scores, axis=-1, keepdims=True) * SCALE
        exponent = jnp.exp2(scores * SCALE - largest)
        return exponent.astype(BF16), jnp.sum(exponent, axis=-1, keepdims=True), largest

    def ratio_of(weights, total, largest):
        weighted = jnp.dot(weights, value_rows, preferred_element_type=F32)
        return (weighted / total).astype(BF16), largest + jnp.log2(total)

    ahead, waiting, ratios, levels = scores_of(*chains[0]), None, {}, {}

    def settle():
        first, m = waiting[0]
        ratio, level = ratio_of(*waiting[1])
        for inner in range(0, CHAIN, block):
            head = (first + inner) // block
            ratios[head, m] = ratio[inner : inner + block]
            levels[head, m] = level[inner : inner + block]

    for number, chain in enumerate(chains):
        scores = ahead
        if number + 1 < len(chains):
            ahead = scores_of(*chains[number + 1])
        exponent = exponent_of(scores)
        if waiting is not None:
            settle()
        waiting = (chain, exponent)
    settle()

    stat_lane = lax.broadcasted_iota(jnp.int32, (block, HV), 1)
    stats = jnp.zeros((block, HV), F32)
    for (head, m), ratio in ratios.items():
        index = 2 * head + m
        for p in range(peers):
            out_ref[p, index * ROWS : (index + 1) * ROWS, :] = ratio[p * ROWS : (p + 1) * ROWS]
        wide = jnp.broadcast_to(levels[head, m], (block, HV))
        stats = jnp.where(stat_lane == index, wide, stats)
    high, middle, low = three_parts(jnp.transpose(stats)[:STATS])
    row = lax.broadcasted_iota(jnp.int32, (STATS, ROWS), 0)
    own_lambda = jnp.zeros((STATS, ROWS), F32)
    if with_gate:
        for part, piece in enumerate(three_parts(jnp.full((STATS, ROWS), lambda_ref[0], F32))):
            own_lambda = jnp.where(row == part, piece, own_lambda)
    stat_row = out_ref.shape[1] - 2 * STATS
    for p in range(peers):
        lanes = slice(p * ROWS, (p + 1) * ROWS)
        if with_gate:
            out_ref[p, GATE_ROW:stat_row, :] = gate_ref[lanes, :]
        upper = jnp.concatenate([high[:, lanes], middle[:, lanes]], axis=1)
        lower = jnp.concatenate([low[:, lanes], own_lambda], axis=1)
        out_ref[p, stat_row:, :] = jnp.concatenate([upper, lower], axis=0).astype(BF16)


def finish_kernel(
    core_ref, first_ref, second_ref, own_ref, other_ref, sums_ref, post_gain_ref, head_gain_ref,
    out_ref, branch_ref, projected_ref,
):
    step = pl.program_id(0)

    @pl.when(step == 0)
    def _():
        levels, lambdas = [], []
        for t in range(TP):
            both = []
            for parts_ref in (first_ref, second_ref):
                stats = parts_ref[t, parts_ref.shape[1] - 2 * STATS :, :].astype(F32)
                upper, lower = stats[:STATS], stats[STATS:]
                level = upper[:, :ROWS] + upper[:, ROWS:] + lower[:, :ROWS]
                both.append(level[:PARTS])
                if parts_ref is first_ref:
                    lambdas.append(lower[0:1, ROWS:] + lower[1:2, ROWS:] + lower[2:3, ROWS:])
            levels.append(jnp.concatenate(both, axis=0))
        shares = []
        for g in range(TP // GROUP):
            group = levels[g * GROUP : (g + 1) * GROUP]
            top = jnp.maximum(jnp.maximum(group[0], group[1]), jnp.maximum(group[2], group[3]))
            group = [jnp.exp2(level - top) for level in group]
            total = group[0] + group[1] + group[2] + group[3]
            shares = shares + [share / total for share in group]
        columns = jnp.concatenate(shares + lambdas, axis=0)
        columns = jnp.concatenate([columns, jnp.zeros_like(columns)], axis=1)
        columns = jnp.concatenate(
            [columns, jnp.zeros((HV - columns.shape[0], HV), F32)], axis=0
        )
        columns = jnp.transpose(columns)[:ROWS]
        for head in range(TP):
            g, j = head // GROUP, head % GROUP
            ratios = []
            for m in range(2):
                index = 2 * j + m
                ratio = jnp.zeros((ROWS, HV), F32)
                parts_ref = first_ref if index < PARTS else second_ref
                first = index % PARTS * ROWS
                for t in range(g * GROUP, (g + 1) * GROUP):
                    part = parts_ref[t, first : first + ROWS, :].astype(F32)
                    column = t * STATS + index
                    ratio = ratio + columns[:, column : column + 1] * part
                ratios.append(ratio)
            column = TP * STATS + head
            attended = ratios[0] - columns[:, column : column + 1] * ratios[1]
            square = jnp.mean(attended * attended, axis=-1, keepdims=True)
            gate = first_ref[head, GATE_ROW : GATE_ROW + ROWS, :].astype(F32)
            branch = attended * lax.rsqrt(square + NORM_EPSILON) * head_gain_ref[...] * silu(gate)
            branch_ref[g, :, j * HV : (j + 1) * HV] = branch.astype(BF16)

    own = core_ref[0]
    pieces = own_ref.shape[0]
    for piece in range(pieces):
        projected = jnp.dot(branch_ref[own], own_ref[piece], preferred_element_type=F32)
        projected = projected + jnp.dot(
            branch_ref[1 - own], other_ref[piece], preferred_element_type=F32
        )
        projected_ref[step * pieces + piece] = projected.astype(BF16).astype(F32)

    @pl.when(step == pl.num_programs(0) - 1)
    def _():
        square = jnp.zeros((ROWS, 1), F32)
        for t in range(TP):
            square = square + jnp.sum(projected_ref[t] * projected_ref[t], axis=-1, keepdims=True)
        factor = lax.rsqrt(square / D + NORM_EPSILON)
        out_gate = vector_of(sums_ref, 2)
        gain = post_gain_ref[...]
        width = D // TP
        for t in range(TP):
            columns = slice(t * width, (t + 1) * width)
            value = projected_ref[t] * factor * gain[:, columns] * out_gate[:, columns]
            out_ref[:, columns] = value.astype(BF16)


def whole_block(shape):
    return pl.BlockSpec(shape, lambda *_: (0,) * len(shape))


def attend(queries, key_values, half, params, extra):
    rows = GATE_ROW + (ROWS if extra else 0) + 2 * STATS
    extra_specs = [
        pl.BlockSpec(memory_space=pltpu.SMEM), pl.BlockSpec((PEERS * ROWS, HV), lambda i: (i, 0))
    ]
    return pl.pallas_call(
        functools.partial(attention_kernel, bool(extra)),
        grid=(TP // PEERS,),
        in_specs=(extra_specs if extra else [])
        + [
            pl.BlockSpec((GROUP // 2, PEERS * ROWS, HV), lambda i: (half, i, 0)),
            whole_block((KEYS, 2 * HV)),
        ],
        out_specs=pl.BlockSpec((PEERS, rows, HV), lambda i: (i, 0, 0)),
        out_shape=jax.ShapeDtypeStruct((TP, rows, HV), BF16),
        compiler_params=params,
        name="attention",
    )(*extra, queries, key_values)


def compute(
    latents, condition, context, context_cond, shift_weight, scale_weight, out_gate_weight,
    pre_gain, post_gain, query_weight, key_weight, value_weight, head_gate_weight,
    lambdas, head_gain, out_weight,
):
    params = pltpu.CompilerParams(vmem_limit_bytes=VMEM_LIMIT)
    both_axes = ("sp", "tp")
    t = lax.axis_index("tp")
    core = lax.axis_index("dp") % 2
    rows = lax.all_gather(latents[0], "tp", axis=0, tiled=False)
    other_context = lax.ppermute(
        context[0], "tp", [(i, (i + GROUP) % TP) for i in range(TP)]
    )
    partials = pl.pallas_call(
        partial_sums_kernel,
        out_shape=jax.ShapeDtypeStruct((SP * TP, 1, CHUNK), F32),
        compiler_params=params,
        name="partial_sums",
    )(condition, context_cond[None, :], shift_weight, scale_weight, out_gate_weight)
    pieces = lax.all_to_all(partials, both_axes, split_axis=0, concat_axis=0, tiled=True)
    own_sums = jnp.sum(pieces, axis=0, keepdims=True)
    copies = jnp.broadcast_to(own_sums, pieces.shape)
    sums = lax.all_to_all(copies, both_axes, split_axis=0, concat_axis=0, tiled=True)
    half = lax.dynamic_slice_in_dim(out_weight, core * GROUP * HV, GROUP * HV, 0)
    half = half + (own_sums[0, 0, 0] * 0.0).astype(BF16)
    own_half = lax.all_gather(half, "tp", axis=0, tiled=False)
    other_half = lax.ppermute(own_half, "dp", [(i, i ^ 1) for i in range(8)])
    place = jnp.stack([t % GROUP, t // GROUP]).astype(jnp.int32)
    queries, head_gate, key_values = pl.pallas_call(
        project_kernel,
        grid_spec=pltpu.PrefetchScalarGridSpec(
            num_scalar_prefetch=1,
            grid=(TP // PROJECT_PIECES,),
            in_specs=[
                pl.BlockSpec((PROJECT_PIECES, ROWS, D), lambda i, _: (i, 0, 0)),
                whole_block((CTX_ROWS, D)),
                whole_block((CTX_ROWS, D)),
                whole_block((SP * TP, 1, CHUNK)),
                whole_block((1, D)),
                whole_block((D, HV)),
                whole_block((D, HV)),
                pl.BlockSpec((D, HV), lambda i, place_ref: (0, place_ref[1])),
                pl.BlockSpec((D, HV), lambda i, place_ref: (0, place_ref[1])),
            ],
            out_specs=[
                whole_block((GROUP, TP * ROWS, HV)),
                whole_block((TP * ROWS, HV)),
                whole_block((QUARTER, 2 * HV)),
            ],
            scratch_shapes=[pltpu.VMEM((PROJECT_PIECES * ROWS, D), BF16)],
        ),
        out_shape=[
            jax.ShapeDtypeStruct((GROUP, TP * ROWS, HV), BF16),
            jax.ShapeDtypeStruct((TP * ROWS, HV), BF16),
            jax.ShapeDtypeStruct((QUARTER, 2 * HV), BF16),
        ],
        compiler_params=params,
        name="project",
    )(
        place, rows, context[0], other_context, sums, pre_gain[None, :],
        query_weight, head_gate_weight, key_weight, value_weight,
    )
    key_values = lax.all_gather(key_values, "sp", axis=0, tiled=True)
    queries = lax.all_to_all(
        queries, "tp", split_axis=0, concat_axis=0, axis_index_groups=TP_GROUPS, tiled=True
    )
    first_parts = attend(queries, key_values, 0, params, (lambdas, head_gate))
    first_parts = lax.all_to_all(first_parts, "tp", split_axis=0, concat_axis=0, tiled=True)
    second_parts = attend(queries, key_values, 1, params, ())
    second_parts = lax.all_to_all(second_parts, "tp", split_axis=0, concat_axis=0, tiled=True)
    weight_block = pl.BlockSpec((FINISH_PIECES, GROUP * HV, D // TP), lambda i, _: (i, 0, 0))
    mixed_out = pl.pallas_call(
        finish_kernel,
        grid_spec=pltpu.PrefetchScalarGridSpec(
            num_scalar_prefetch=1,
            grid=(TP // FINISH_PIECES,),
            in_specs=[
                whole_block(first_parts.shape),
                whole_block(second_parts.shape),
                weight_block,
                weight_block,
                whole_block((SP * TP, 1, CHUNK)),
                whole_block((1, D)),
                whole_block((1, HV)),
            ],
            out_specs=whole_block((ROWS, D)),
            scratch_shapes=[
                pltpu.VMEM((2, ROWS, GROUP * HV), BF16),
                pltpu.VMEM((TP, ROWS, D // TP), F32),
            ],
        ),
        out_shape=jax.ShapeDtypeStruct((ROWS, D), BF16),
        compiler_params=params,
        name="finish",
    )(
        core.astype(jnp.int32)[None], first_parts, second_parts, own_half, other_half, sums,
        post_gain[None, :], head_gain[None, :],
    )
    return mixed_out[None]


def solution(mesh):
    tokens = P("dp", ("sp", "tp"), None)
    channels = P(("sp", "tp"), None)
    return jax.shard_map(
        compute,
        mesh=mesh,
        in_specs=(
            tokens, P("dp", ("sp", "tp")), tokens, P(("sp", "tp")), channels, channels, channels,
            P(), P(), P(None, "tp"), P(), P(), P(None, "tp"), P("tp"), P(), P(None, "tp"),
        ),
        out_specs=tokens,
        check_vma=False,
    )
```
